32 devices in a mesh: grp: 2 (over y), fs: 4 (over z), tp: 4 (over x, core).
Axes of the slice: x: 2, y: 2, z: 4, core: 2. Of those that a mesh axis runs over, the one named last changes fastest.
Arguments:
- tokens: bfloat16 [8192, 2048], P(('grp', 'fs'), 'tp'), parts along dimension 0, may hold values from -6 to 6
- norm1_gain: float32 [2048], replicated, may hold values from 0.1 to 1.9
- weight_u: float32 [2048, 1024], P('fs', 'tp'), may hold values from -0.125 to 0.125
- weight_v: float32 [2048, 1024], P('fs', 'tp'), may hold values from -0.125 to 0.125
- scale_u: float32 [1024], P('tp'), may hold values from 0.5 to 2
- scale_v: float32 [1024], P('tp'), may hold values from 0.05 to 4.5
- mix_gain: float32 [1024], P('tp'), may hold values from 0.1 to 1.9
- spatial_weight: float32 [4, 128, 128], replicated, may hold values from -0.5 to 0.5
- spatial_bias: float32 [4, 128], replicated, may hold values from 0.5 to 1.5
- weight_out: float32 [1024, 2048], P('tp', 'fs'), may hold values from -0.1875 to 0.1875
- scale_out: float32 [2048], P('fs'), may hold values from 0.5 to 2
- norm2_gain: float32 [2048], replicated, may hold values from 0.1 to 1.9
- weight_up: float32 [2048, 8192], P('fs', 'tp'), may hold values from -0.125 to 0.125
- scale_up: float32 [8192], P('tp'), may hold values from 0.5 to 2
- weight_down: float32 [8192, 2048], P('tp', 'fs'), may hold values from -0.0625 to 0.0625
- scale_down: float32 [2048], P('fs'), may hold values from 0.5 to 2
Outputs:
- result: bfloat16 [8192, 2048], P(('grp', 'fs'), 'tp'), parts along dimension 0
The draws below stay inside these ranges and needn't reach their ends.
There are 2 independent parts, one for each index of `grp`. The reference program is written for one: setup_inputs(seed, part) draws one part's arguments, and reference() takes and returns one part's arrays. A program takes and returns all parts, laid end to end along the dimension named above; an argument that names none is the same for every part. Nothing has to cross between parts.
All inputs are finite; a program needn't handle non-finite values.
Results may differ from the reference program's by a relative error of at most 0.023.
Values may be sent and summed in bfloat16 or wider, within the bound.
A program may use at most 128 MiB of HBM per device.

```python
import math
import jax
import jax.numpy as jnp
from jax import lax

D = 2048
GM_W = 1024
GROUPS = 4
BLOCK = 128
FF = 8192
TOKENS = 4096
N_TP = 4


def draw_scale_v(key, part):
    columns = jnp.arange(GM_W, dtype=jnp.float32) / GM_W
    roughness = jax.random.uniform(key, (GM_W,), jnp.float32, 0.5, 1.5)
    return 0.4 * jnp.exp(columns * jnp.log(4.0)) * roughness


def level_of(stream_key, dims, split, least, top_value):
    gain, own = 1.0, jax.random.fold_in(stream_key, 6)
    for axis_at, blocks in split:
        heights = jnp.exp(jax.random.uniform(jax.random.fold_in(own, axis_at), (blocks,), jnp.float32, least / len(split), top_value / len(split)))
        gain = gain * jnp.repeat(heights, dims[axis_at] // blocks).reshape([-1 if axis == axis_at else 1 for axis in range(len(dims))])
    return gain


def bell_draw(stream_key, dims, spread, limit, cuts=(), kind=jnp.bfloat16):
    entries = spread * jax.random.normal(stream_key, dims, jnp.float32)
    if cuts:
        entries = entries * level_of(stream_key, dims, cuts, -0.22, 0.18)
    return jnp.clip(entries, -limit, limit).astype(kind)


def setup_inputs(seed: int = 0, part: int = 0) -> dict:
    seeds = jax.random.split(jax.random.key(seed), 17)
    part_keys = jax.random.split(jax.random.fold_in(seeds[16], part), 17)
    tokens = bell_draw(part_keys[0], (TOKENS, D), 1.0, 6.0, ((0, 4), (1, 4)))
    norm1_gain = jnp.clip(1.0 + 0.18 * jax.random.normal(seeds[1], (D,), jnp.float32), 0.1, 1.9)
    weight_u = bell_draw(seeds[2], (D, GM_W), D ** -0.5, 0.125, ((0, 4), (1, 4)), jnp.float32)
    weight_v = bell_draw(seeds[3], (D, GM_W), D ** -0.5, 0.125, ((0, 4), (1, 4)), jnp.float32)
    scale_u = jnp.clip(jnp.exp(math.log(2.0) - 1.3862944 * jax.random.uniform(seeds[4], (GM_W,), jnp.float32) ** level_of(seeds[4], (GM_W,), ((0, 4),), -0.2, 0.2)), 0.5, 2.0)
    scale_v = draw_scale_v(jax.random.fold_in(seeds[16], 71), part)
    mix_gain = jnp.clip(1.0 + 0.18 * jax.random.normal(seeds[6], (GM_W,), jnp.float32), 0.1, 1.9)
    spatial_weight = bell_draw(seeds[7], (GROUPS, BLOCK, BLOCK), BLOCK ** -0.5, 0.5, (), jnp.float32)
    spatial_bias = jnp.clip(jax.random.uniform(seeds[8], (GROUPS, BLOCK), jnp.float32, 0.5, 1.5), 0.5, 1.5)
    weight_out = bell_draw(seeds[9], (GM_W, D), GM_W ** -0.5, 0.1875, ((0, 4), (1, 4)), jnp.float32)
    scale_out = jnp.clip(jnp.exp(math.log(2.0) - 1.3862944 * jax.random.uniform(seeds[10], (D,), jnp.float32) ** level_of(seeds[10], (D,), ((0, 4),), -0.2, 0.2)), 0.5, 2.0)
    norm2_gain = jnp.clip(1.0 + 0.18 * jax.random.normal(seeds[11], (D,), jnp.float32), 0.1, 1.9)
    weight_up = bell_draw(seeds[12], (D, FF), D ** -0.5, 0.125, ((0, 4), (1, 4)), jnp.float32)
    scale_up = jnp.clip(jnp.exp(math.log(2.0) - 1.3862944 * jax.random.uniform(seeds[13], (FF,), jnp.float32) ** level_of(seeds[13], (FF,), ((0, 4),), -0.2, 0.2)), 0.5, 2.0)
    weight_down = bell_draw(seeds[14], (FF, D), FF ** -0.5, 0.0625, ((0, 4), (1, 4)), jnp.float32)
    scale_down = jnp.clip(jnp.exp(math.log(2.0) - 1.3862944 * jax.random.uniform(seeds[15], (D,), jnp.float32) ** level_of(seeds[15], (D,), ((0, 4),), -0.2, 0.2)), 0.5, 2.0)
    return {"tokens": tokens, "norm1_gain": norm1_gain, "weight_u": weight_u, "weight_v": weight_v, "scale_u": scale_u, "scale_v": scale_v, "mix_gain": mix_gain, "spatial_weight": spatial_weight, "spatial_bias": spatial_bias, "weight_out": weight_out, "scale_out": scale_out, "norm2_gain": norm2_gain, "weight_up": weight_up, "scale_up": scale_up, "weight_down": weight_down, "scale_down": scale_down}


def rms_rows(values, gain_vector):
    widened = values.astype(jnp.float32)
    scaled = widened * lax.rsqrt(lax.optimization_barrier(jnp.mean(widened * widened, axis=-1, keepdims=True)) + 1e-06)
    return (scaled * gain_vector).astype(jnp.bfloat16)

def run_sum(operand_left, operand_right, column_scale, pieces):
    run_width = operand_left.shape[1] // pieces
    running = jnp.zeros((operand_left.shape[0], operand_right.shape[1]), jnp.float32)
    for run_index in range(pieces):
        lower = run_index * run_width
        partial_term = jnp.dot(operand_left[:, lower:lower + run_width], operand_right[lower:lower + run_width], preferred_element_type=jnp.float32) * column_scale
        running = running + lax.optimization_barrier(partial_term.astype(jnp.bfloat16)).astype(jnp.float32)
    return running

def reference(tokens, norm1_gain, weight_u, weight_v, scale_u, scale_v, mix_gain, spatial_weight, spatial_bias, weight_out, scale_out, norm2_gain, weight_up, scale_up, weight_down, scale_down):
    normed_in = rms_rows(tokens, norm1_gain)
    pre_u = jnp.dot(normed_in, weight_u.astype(jnp.bfloat16), preferred_element_type=jnp.float32) * scale_u
    pre_v = jnp.dot(normed_in, weight_v.astype(jnp.bfloat16), preferred_element_type=jnp.float32) * scale_v
    gate_u = jax.nn.gelu(pre_u)
    act_v = jax.nn.gelu(pre_v)
    row_mean = lax.optimization_barrier(jnp.mean(act_v, axis=-1, keepdims=True))
    square = lax.optimization_barrier(jnp.mean(act_v * act_v, axis=-1, keepdims=True))
    v_norm = ((act_v - row_mean) * lax.rsqrt(square - row_mean * row_mean + 1e-06) * mix_gain).astype(jnp.bfloat16)
    lower_mask = jnp.tril(jnp.ones((BLOCK, BLOCK), jnp.float32))
    spatial_mask = (spatial_weight * lower_mask).astype(jnp.bfloat16)
    blocks = v_norm.reshape(TOKENS // BLOCK, BLOCK, GROUPS, GM_W // GROUPS)
    mixed_cols = jnp.einsum('gts,nsgc->ntgc', spatial_mask.astype(jnp.float32), blocks.astype(jnp.float32))
    mixed_cols = mixed_cols + spatial_bias.T[None, :, :, None]
    gated = (gate_u * mixed_cols.reshape(TOKENS, GM_W)).astype(jnp.bfloat16)
    mixer_sum = run_sum(gated, weight_out.astype(jnp.bfloat16), scale_out, N_TP)
    residual = (tokens.astype(jnp.float32) + mixer_sum).astype(jnp.bfloat16)
    normed_mid = rms_rows(residual, norm2_gain)
    pre_up = jnp.dot(normed_mid, weight_up.astype(jnp.bfloat16), preferred_element_type=jnp.float32) * scale_up
    hidden = jnp.square(jax.nn.relu(pre_up)).astype(jnp.bfloat16)
    channel_sum = run_sum(hidden, weight_down.astype(jnp.bfloat16), scale_down, N_TP)
    return (residual.astype(jnp.float32) + channel_sum).astype(jnp.bfloat16)
```

```python
import jax
import jax.numpy as jnp
from jax import lax
from jax.experimental import pallas as pl
from jax.experimental.pallas import tpu as pltpu
from jax.sharding import PartitionSpec as P

GM_W = 1024
GROUPS = 4
BLOCK = 128


def swap(value, axis, size, mask):
    return lax.ppermute(value, axis, [(k, k ^ mask) for k in range(size)])


def over_fs(piece, fs, relay, near_too):
    if fs != 4 or not relay:
        return [piece] + [swap(piece, "fs", fs, mask) for mask in range(1, fs)]
    far = swap(piece, "fs", 4, 2)
    near = swap(piece, "fs", 4, 1) if near_too else None
    middle = lax.ppermute(piece, "fs", [(1, 2), (2, 1)])
    relayed = lax.ppermute(far, "fs", [(1, 0), (2, 3)])
    me = lax.axis_index("fs")
    last = jnp.where((me == 1) | (me == 2), middle, relayed)
    return [piece, near, far, last]


def gather_weight(shard, cut_axis, fs, relay=False, whole_near=False):
    half = shard.shape[cut_axis] // 2
    group = lax.axis_index("grp")
    mine = lax.dynamic_slice_in_dim(shard, group * half, half, cut_axis)
    other = lax.dynamic_slice_in_dim(shard, (1 - group) * half, half, cut_axis)
    whole_near = whole_near and relay and fs == 4
    firsts = over_fs(mine, fs, relay, not whole_near)
    if whole_near:
        near = swap(jnp.concatenate([mine, other], axis=cut_axis), "fs", fs, 1)
        firsts[1], near_other = jnp.split(near, 2, axis=cut_axis)
    seconds = [other] + [
        near_other
        if whole_near and mask == 1
        else lax.ppermute(firsts[mask], "grp", [(0, 1), (1, 0)])
        for mask in range(1, fs)
    ]
    return firsts, seconds


def halves_swapped(value, axis):
    half = value.shape[axis] // 2
    group = lax.axis_index("grp")
    return jnp.concatenate(
        [
            lax.dynamic_slice_in_dim(value, group * half, half, axis),
            lax.dynamic_slice_in_dim(value, (1 - group) * half, half, axis),
        ],
        axis=axis,
    )


def gather_rows(piece, tp):
    blocks = [None] * tp
    blocks[0] = piece
    bit = tp // 2
    while bit:
        for at in range(tp):
            if blocks[at] is not None and not at & bit and blocks[at | bit] is None:
                blocks[at | bit] = "due"
        for at in range(tp):
            if isinstance(blocks[at], str):
                blocks[at] = swap(blocks[at ^ bit], "tp", tp, bit)
        bit //= 2
    return blocks


def normed_blocks(blocks, gain, fs, tp):
    feature_count = gain.shape[0]
    width, fine = feature_count // tp, feature_count // fs
    squares = sum(
        jnp.sum(jnp.square(block.astype(jnp.float32)), axis=1) for block in blocks
    )
    inverse = lax.rsqrt(squares / feature_count + 1e-06)[:, None]
    stacked = jnp.stack(blocks)
    me_fs, me_tp = lax.axis_index("fs"), lax.axis_index("tp")
    pieces = []
    for mask in range(fs):
        block = me_fs ^ mask
        first = block * fine
        whole = lax.dynamic_index_in_dim(stacked, (first // width) ^ me_tp, 0, keepdims=False)
        if fine != width:
            whole = lax.dynamic_slice_in_dim(whole, first % width, fine, 1)
        gain_piece = lax.dynamic_slice_in_dim(gain, first, fine, 0)
        pieces.append((whole.astype(jnp.float32) * inverse * gain_piece).astype(jnp.bfloat16))
    return jnp.concatenate(pieces, axis=1)


def scatter_sum(terms, fs, tp):
    stacked = jnp.stack(terms)
    ratio = fs // tp
    me_fs, me_tp = lax.axis_index("fs"), lax.axis_index("tp")
    sums = []
    for mask in range(tp):
        parts = [
            lax.dynamic_index_in_dim(
                stacked, ((me_tp ^ mask) * ratio + at) ^ me_fs, 0, keepdims=False
            )
            for at in range(ratio)
        ]
        sums.append(parts[0] if ratio == 1 else jnp.concatenate(parts, axis=1))
    bit = 1
    while bit < tp:
        kept = {}
        for at in range(tp):
            if sums[at] is not None and not at & bit:
                got = swap(sums[at | bit].astype(jnp.bfloat16), "tp", tp, bit)
                kept[at] = sums[at].astype(jnp.float32) + got.astype(jnp.float32)
        sums = [kept.get(at) for at in range(tp)]
        bit *= 2
    return sums[0]


def make(fs, tp):
    def layer(
        tokens,
        norm1_gain,
        weight_u,
        weight_v,
        scale_u,
        scale_v,
        mix_gain,
        spatial_weight,
        spatial_bias,
        weight_out,
        scale_out,
        norm2_gain,
        weight_up,
        scale_up,
        weight_down,
        scale_down,
    ):
        half = weight_u.shape[1] // 2
        token_blocks = gather_rows(tokens, tp)
        both = jnp.stack([weight_u, weight_v], axis=1).astype(jnp.bfloat16)
        both_mine, both_other = gather_weight(both, 2, fs)
        scales = jnp.stack([scale_out, scale_down])
        all_scales = [scales] + [swap(scales, "fs", fs, mask) for mask in range(1, fs)]
        out_mine, out_other = gather_weight(weight_out.astype(jnp.bfloat16), 0, fs)
        up_mine, up_other = gather_weight(weight_up.astype(jnp.bfloat16), 1, fs, relay=True)
        down_mine, down_other = gather_weight(weight_down.astype(jnp.bfloat16), 0, fs, relay=True, whole_near=True)

        normed_in = normed_blocks(token_blocks, norm1_gain, fs, tp)
        full_u = jnp.concatenate(
            [jnp.concatenate([a[:, 0], b[:, 0]], axis=1) for a, b in zip(both_mine, both_other)]
        )
        full_v = jnp.concatenate(
            [jnp.concatenate([a[:, 1], b[:, 1]], axis=1) for a, b in zip(both_mine, both_other)]
        )
        pre_v = jnp.dot(normed_in, full_v, preferred_element_type=jnp.float32)
        pre_u = jnp.dot(normed_in, full_u, preferred_element_type=jnp.float32)
        act_v = jax.nn.gelu(pre_v * halves_swapped(scale_v, 0))
        gate_u = jax.nn.gelu(pre_u * halves_swapped(scale_u, 0))
        local_width = 2 * half
        row_sums, row_squares = lax.psum(
            (jnp.sum(act_v, axis=1), jnp.sum(act_v * act_v, axis=1)), "tp"
        )
        row_mean = (row_sums / GM_W)[:, None]
        square = (row_squares / GM_W)[:, None]
        v_norm = (
            (act_v - row_mean)
            * lax.rsqrt(square - row_mean * row_mean + 1e-06)
            * halves_swapped(mix_gain, 0)
        ).astype(jnp.bfloat16)
        group_index = lax.axis_index("tp") * local_width // (GM_W // GROUPS)
        lower_mask = jnp.tril(jnp.ones((BLOCK, BLOCK), jnp.float32))
        spatial_mask = (
            lax.dynamic_index_in_dim(spatial_weight, group_index, 0, keepdims=False) * lower_mask
        ).astype(jnp.bfloat16)
        block_bias = lax.dynamic_index_in_dim(spatial_bias, group_index, 0, keepdims=False)
        blocks = v_norm.reshape(-1, BLOCK, local_width)
        mixed = jnp.einsum("ts,nsc->ntc", spatial_mask, blocks, preferred_element_type=jnp.float32)
        mixed = mixed + block_bias[None, :, None]
        gated = (gate_u * mixed.reshape(-1, local_width)).astype(jnp.bfloat16)

        terms = []
        for a, b, scale in zip(out_mine, out_other, all_scales):
            product = jnp.dot(gated, jnp.concatenate([a, b]), preferred_element_type=jnp.float32)
            terms.append((product * scale[0]).astype(jnp.bfloat16))
        mixer_sum = scatter_sum(terms, fs, tp)
        residual = (tokens.astype(jnp.float32) + mixer_sum).astype(jnp.bfloat16)

        normed_mid = normed_blocks(gather_rows(residual, tp), norm2_gain, fs, tp)
        full_up = jnp.concatenate(
            [jnp.concatenate([a, b], axis=1) for a, b in zip(up_mine, up_other)]
        )
        pre_up = jnp.dot(normed_mid, full_up, preferred_element_type=jnp.float32)
        hidden = jnp.square(jax.nn.relu(pre_up * halves_swapped(scale_up, 0))).astype(jnp.bfloat16)
        terms = []
        for a, b, scale in zip(down_mine, down_other, all_scales):
            product = jnp.dot(hidden, jnp.concatenate([a, b]), preferred_element_type=jnp.float32)
            terms.append((product * scale[1]).astype(jnp.bfloat16))
        channel_sum = scatter_sum(terms, fs, tp)
        return (residual.astype(jnp.float32) + channel_sum).astype(jnp.bfloat16)

    return layer


MESH = pl.DeviceIdType.MESH
WAVES = 6
CHUNKS = 4
STEP = 64


def rows_of(first, size, unit):
    return pl.ds(pl.multiple_of(first, unit), size)


def row_loop(first, count, step, body):
    def at(i, carry):
        body(rows_of(first + i * step, step, step))
        return carry

    lax.fori_loop(0, count // step, at, 0)


def matmul(a, b):
    return jnp.dot(a, b, preferred_element_type=jnp.float32)


def fused_kernel(
    tokens, weight_u, weight_v, weight_out, weight_up, weight_down,
    gain1, scale_u, scale_v, mix_gain, spatial_weight, spatial_bias,
    scale_out, scale_down, gain2, scale_up,
    result,
    stage, g_both, g_out, g_up, g_down, tok, mid, normed, hidden,
    act_v, gate_u, gated, stat, stat_rows, scales, terms, core_in, x_out, x_in,
    load_sem, zs, zr, ys, yr, gs, gr, cs, cr, xs, xr, cs2, cr2, xs2, xr2,
    sts, strv, scs, scr,
):
    y, z, t = lax.axis_index("grp"), lax.axis_index("fs"), lax.axis_index("tp")
    other_y = 1 - y
    upper = z // 2
    planes = (z, 1 - z + 4 * upper, 2 - upper, 3 - 3 * upper)
    is_mid = (z == 1) | (z == 2)
    t1 = t + 1 - 2 * (t % 2)
    t2 = (t + 2) % 4
    t3 = (t1 + 2) % 4
    rows, fine = tokens.shape
    chunk = rows // CHUNKS
    width = weight_u.shape[1]
    hid = weight_up.shape[1]
    hhalf = hid // 2
    feature_count = gain1.shape[1]
    sends = []

    def remote(source, target, send, recv, **where):
        return pltpu.make_async_remote_copy(
            src_ref=source, dst_ref=target, send_sem=send, recv_sem=recv,
            device_id=where, device_id_type=MESH,
        )

    barrier = pltpu.get_barrier_semaphore()
    for p in planes[1:]:
        pl.semaphore_signal(barrier, inc=1, device_id={"fs": p}, device_id_type=MESH)
    pl.semaphore_signal(barrier, inc=1, device_id={"grp": other_y}, device_id_type=MESH)
    for u in (t1, t2, t3):
        pl.semaphore_signal(barrier, inc=1, device_id={"tp": u}, device_id_type=MESH)

    def load(source, slot, part=None):
        target = stage.at[slot] if part is None else part
        return pltpu.make_async_copy(source, target, load_sem.at[slot])

    half_w = width
    load_u = load(weight_u, 0, stage.at[0, :, pl.ds(0, half_w)])
    load_v = pltpu.make_async_copy(weight_v, stage.at[0, :, pl.ds(half_w, half_w)], load_sem.at[4])
    load_out = load(weight_out, 1, stage.at[1, pl.ds(0, width), :])
    load_tok = pltpu.make_async_copy(tokens, tok.at[t], load_sem.at[5])

    def load_up(j, slot):
        return load(weight_up.at[:, pl.ds(j * fine, fine)], slot)

    def load_down(j, slot):
        return load(weight_down.at[pl.ds(j * fine, fine), :], slot)

    load_u.start()
    load_v.start()
    load_out.start()
    load_up(0, 2).start()
    load_up(1, 3).start()
    load_tok.start()
    scales[z] = jnp.concatenate([scale_out[...], scale_down[...]], axis=0)

    pl.semaphore_wait(barrier, 7)

    def gather_copies(which, buffer, own_source, r):
        part = pl.ds(r * chunk, chunk)
        to_x = remote(own_source.at[part], buffer.at[t, part], gs.at[which, 0, r], gr.at[which, t, r], tp=t2)
        to_core = remote(own_source.at[part], buffer.at[t, part], gs.at[which, 1, r], gr.at[which, t, r], tp=t1)
        return to_x, to_core

    def gather_start(which, buffer, own_source, r):
        for copy in gather_copies(which, buffer, own_source, r):
            copy.start()
            sends.append(copy)

    def gather_await(which, buffer, block, r):
        part = pl.ds(r * chunk, chunk)
        remote(buffer.at[block, part], buffer.at[block, part], gs.at[which, 2, r], gr.at[which, block, r], tp=t1).wait_recv()

    def gather_relay(which, buffer, r):
        gather_await(which, buffer, t2, r)
        part = pl.ds(r * chunk, chunk)
        copy = remote(buffer.at[t2, part], buffer.at[t2, part], gs.at[which, 2, r], gr.at[which, t2, r], tp=t1)
        copy.start()
        sends.append(copy)

    def piece(w, p, h):
        if w == 0:
            size = fine // 2
            return g_both.at[rows_of(p * fine + h * size, size, size), :]
        if w == 1:
            size = width // 2
            return g_out.at[p, rows_of(h * size, size, size), :]
        if w < 4:
            size = fine // 2
            return g_up.at[h, rows_of(p * fine + (w - 2) * size, size, size), :]
        size = hhalf // 2
        return g_down.at[p, rows_of(h * hhalf + (w - 4) * size, size, size), :]

    def z_copy(w, p, to, slot):
        return remote(piece(w, p, y), piece(w, p, y), zs.at[w, slot], zr.at[w, p], fs=to)

    def y_copy(w, i, h):
        p = planes[i]
        return remote(piece(w, p, h), piece(w, p, h), ys.at[w, i - 1], yr.at[w, p], grp=other_y)

    def own(w):
        z_copy(w, z, planes[1], 0).start()

        @pl.when(is_mid)
        def _():
            z_copy(w, z, planes[2], 1).start()

    def arrive(w, i):
        p = planes[i]
        z_copy(w, p, planes[1], 1 + i).wait_recv()

        @pl.when(is_mid)
        def _():
            z_copy(w, p, planes[2] if i == 1 else planes[1], 1 + i).start()

        y_copy(w, i, y).start()

    def arrive_y(w, i):
        y_copy(w, i, other_y).wait_recv()

    def arrive_all_y(w):
        for i in (1, 2, 3):
            arrive_y(w, i)

    for r in range(CHUNKS):
        gather_start(0, tok, tokens, r)

    def cast_to(slot, count, store):
        row_loop(0, count, STEP, lambda part: store(part, stage[slot, part, :].astype(jnp.bfloat16)))

    def at_offset(part, base):
        return rows_of(part.start + base, part.size, part.size)

    load_u.wait()
    load_v.wait()

    def store_both(part, value):
        g_both[at_offset(part, z * fine), :] = value

    cast_to(0, fine, store_both)
    load_up(2, 0).start()
    load_out.wait()

    def store_out(part, value):
        g_out[z, part, :] = value

    own(0)
    cast_to(1, width, store_out)
    load_up(3, 1).start()
    for i in (1, 2, 3):
        copy = remote(scales.at[z], scales.at[z], scs.at[i - 1], scr.at[z], fs=planes[i])
        copy.start()
        sends.append(copy)

    def cast_up(j, slot):
        load_up(j, slot).wait()
        cols = pl.ds((j % 2) * fine, fine)

        def store(part, value):
            g_up[j // 2, at_offset(part, z * fine), cols] = value

        cast_to(slot, fine, store)

    def cast_down(j, slot):
        load_down(j, slot).wait()

        def store(part, value):
            g_down[z, at_offset(part, j * fine), :] = value

        cast_to(slot, fine, store)

    own(1)
    cast_up(0, 2)
    load_down(0, 2).start()
    gather_relay(0, tok, 0)
    cast_up(1, 3)
    load_down(1, 3).start()
    arrive(0, 1)
    cast_up(2, 0)
    load_down(2, 0).start()
    cast_up(3, 1)
    load_down(3, 1).start()
    arrive(1, 1)
    gather_relay(0, tok, 1)
    arrive(0, 2)
    arrive(1, 2)
    own(2)
    cast_down(0, 2)
    cast_down(1, 3)
    gather_relay(0, tok, 2)
    cast_down(2, 0)
    cast_down(3, 1)
    arrive(0, 3)
    arrive(1, 3)
    own(3)
    load_tok.wait()

    def norm_rows(buffer, gain, first, count):
        def body(part):
            total = jnp.zeros((part.size, 1), jnp.float32)
            for b in range(4):
                value = buffer[b, part, :].astype(jnp.float32)
                total = total + jnp.sum(value * value, axis=1, keepdims=True)
            inverse = lax.rsqrt(total / feature_count + 1e-06)
            for b in range(4):
                value = buffer[b, part, :].astype(jnp.float32)
                cols = pl.ds(b * fine, fine)
                normed[part, cols] = (value * inverse * gain[:, cols]).astype(jnp.bfloat16)

        row_loop(first, count, 32, body)

    def norm_chunk(which, buffer, gain, r):
        gather_await(which, buffer, t1, r)
        gather_await(which, buffer, t3, r)
        norm_rows(buffer, gain, r * chunk, chunk)

    for r in range(CHUNKS):
        if r == CHUNKS - 1:
            gather_relay(0, tok, r)
        norm_chunk(0, tok, gain1, r)

    arrive(2, 1)
    arrive_all_y(0)

    lane = lax.broadcasted_iota(jnp.int32, (chunk, 128), 1)

    def v_chunk(part):
        value = jax.nn.gelu(matmul(normed[part, :], g_both[:, width:]) * scale_v[...])
        act_v[part, :] = value
        total = jnp.sum(value, axis=1, keepdims=True)
        square = jnp.sum(value * value, axis=1, keepdims=True)
        stat[part, :] = jnp.where(lane == 0, total, jnp.where(lane == 1, square, 0.0))

    row_loop(0, rows, chunk, v_chunk)
    stat_rows[0] = stat[...].T[0:8]

    def stat_copy(k, u):
        return remote(stat_rows.at[0], stat_rows.at[k], sts.at[k - 1], strv.at[k], tp=u)

    def u_chunk(part):
        gate_u[part, :] = jax.nn.gelu(matmul(normed[part, :], g_both[:, :width]) * scale_u[...])

    for k, u in ((1, t1), (2, t2), (3, t3)):
        copy = stat_copy(k, u)
        copy.start()
        sends.append(copy)
    row_loop(0, rows, chunk, u_chunk)
    arrive(2, 2)
    for k, u in ((1, t1), (2, t2), (3, t3)):
        stat_copy(k, u).wait_recv()
    totals = stat_rows[0] + stat_rows[1] + stat_rows[2] + stat_rows[3]
    stat[...] = jnp.concatenate([totals, jnp.zeros((120, rows), jnp.float32)], axis=0).T

    down_at = lax.broadcasted_iota(jnp.int32, (BLOCK, BLOCK), 0)
    along = lax.broadcasted_iota(jnp.int32, (BLOCK, BLOCK), 1)
    mask = jnp.where(along <= down_at, spatial_weight[t], 0.0).astype(jnp.bfloat16)
    bias_row = spatial_bias[pl.ds(t, 1), :]
    bias = jnp.sum(jnp.where(along == down_at, bias_row, 0.0), axis=1, keepdims=True)

    def mix_block(part):
        mean = stat[part, 0:1] / GM_W
        square = stat[part, 1:2] / GM_W
        v_norm = (act_v[part, :] - mean) * lax.rsqrt(square - mean * mean + 1e-06) * mix_gain[...]
        mixed = matmul(mask, v_norm.astype(jnp.bfloat16)) + bias
        gated[part, :] = (gate_u[part, :] * mixed).astype(jnp.bfloat16)

    row_loop(0, rows, BLOCK, mix_block)
    arrive_all_y(1)
    for i in (1, 2, 3):
        remote(scales.at[planes[i]], scales.at[planes[i]], scs.at[i - 1], scr.at[planes[i]], fs=planes[i]).wait_recv()

    def core_copy(k, block, r):
        part = pl.ds(r * chunk, chunk)
        return remote(terms.at[block, part], core_in.at[k, part], cs.at[k, r], cr.at[k, r], tp=t1)

    def x_copy(send, recv, r):
        part = pl.ds(r * chunk, chunk)
        return remote(x_out.at[part], x_in.at[part], send.at[r], recv.at[r], tp=t2)

    mix_sends = []
    for r in range(CHUNKS):
        part = pl.ds(r * chunk, chunk)
        for j in range(4):
            product = matmul(gated[part, :], g_out[j])
            terms[j, part, :] = (product * scales[j, 0:1, :]).astype(jnp.bfloat16)
        for k, block in ((0, t1), (1, t3)):
            copy = core_copy(k, block, r)
            copy.start()
            mix_sends.append(copy)

    def pair_out(block, slot, r):
        def body(part):
            both = terms[block, part, :].astype(jnp.float32) + core_in[slot, part, :].astype(jnp.float32)
            x_out[part, :] = both.astype(jnp.bfloat16)

        row_loop(r * chunk, chunk, STEP, body)

    for r in range(CHUNKS):
        core_copy(0, t1, r).wait_recv()
        core_copy(1, t3, r).wait_recv()
        pair_out(t2, 1, r)
        copy = x_copy(xs, xr, r)
        copy.start()
        mix_sends.append(copy)
    own(4)
    arrive(2, 3)

    for r in range(CHUNKS):
        x_copy(xs, xr, r).wait_recv()

        def residual_rows(part):
            total = terms[t, part, :].astype(jnp.float32) + core_in[0, part, :].astype(jnp.float32)
            total = total + x_in[part, :].astype(jnp.float32)
            mid[t, part, :] = (tok[t, part, :].astype(jnp.float32) + total).astype(jnp.bfloat16)

        row_loop(r * chunk, chunk, STEP, residual_rows)
        gather_start(1, mid, mid.at[t], r)
        if r == 1:
            arrive(3, 1)
    arrive(3, 2)
    for copy in mix_sends:
        copy.wait_send()
    own(5)
    for r in range(CHUNKS):
        gather_relay(1, mid, r)
        if r == 2:
            arrive(3, 3)
        if r > 0:
            norm_chunk(1, mid, gain2, r - 1)
    norm_chunk(1, mid, gain2, CHUNKS - 1)

    tile = min(hhalf, fine)

    def up_half(h):
        def body(part):
            for n in range(hhalf // tile):
                cols = pl.ds(n * tile, tile)
                place = rows_of(h * hhalf + n * tile, tile, 128)
                value = matmul(normed[part, :], g_up[h, :, cols]) * scale_up[:, place]
                value = jnp.maximum(value, 0.0)
                hidden[part, place] = (value * value).astype(jnp.bfloat16)

        row_loop(0, rows, chunk, body)

    arrive(4, 1)
    up_half(y)
    arrive(4, 2)
    arrive_all_y(2)
    arrive_all_y(3)
    up_half(other_y)
    arrive(4, 3)

    def chan_core(i, r):
        j = planes[i]
        part = rows_of(r * chunk, chunk, chunk)
        return remote(terms.at[j, part], core_in.at[j // 2, part], cs2.at[i, r], cr2.at[j // 2, r], tp=t1)

    def down_piece(i):
        j = planes[i]
        mine = (j % 2) == (t % 2)

        def one(r, carry):
            part = rows_of(r * chunk, chunk, chunk)
            product = matmul(hidden[part, :], g_down[j])
            terms[j, part, :] = (product * scales[j, 1:2, :]).astype(jnp.bfloat16)

            @pl.when(jnp.logical_not(mine))
            def _():
                chan_core(i, r).start()

            return carry

        lax.fori_loop(0, CHUNKS, one, 0)

        @pl.when(mine)
        def _():
            for r in range(CHUNKS):
                chan_core(i, r).wait_recv()

                @pl.when(j != t)
                def _():
                    pair_out(j, j // 2, r)
                    x_copy(xs2, xr2, r).start()

    down_piece(0)
    arrive(5, 1)
    arrive_y(4, 1)
    arrive(5, 2)
    arrive_y(5, 1)
    down_piece(1)
    arrive(5, 3)
    arrive_y(4, 2)
    arrive_y(5, 2)
    down_piece(2)
    arrive_y(4, 3)
    arrive_y(5, 3)
    down_piece(3)

    for r in range(CHUNKS):
        x_copy(xs2, xr2, r).wait_recv()

        def result_rows(part):
            total = terms[t, part, :].astype(jnp.float32) + core_in[t // 2, part, :].astype(jnp.float32)
            total = total + x_in[part, :].astype(jnp.float32)
            result[part, :] = (mid[t, part, :].astype(jnp.float32) + total).astype(jnp.bfloat16)

        row_loop(r * chunk, chunk, STEP, result_rows)

    for copy in sends:
        copy.wait_send()
    for w in range(WAVES):
        z_copy(w, z, planes[1], 0).wait_send()
        for i in (1, 2, 3):
            y_copy(w, i, y).wait_send()
    for r in range(CHUNKS):
        x_copy(xs2, xr2, r).wait_send()
    for i in range(4):
        @pl.when((planes[i] % 2) != (t % 2))
        def _():
            for r in range(CHUNKS):
                chan_core(i, r).wait_send()

    @pl.when(is_mid)
    def _():
        for w in range(WAVES):
            z_copy(w, z, planes[2], 1).wait_send()
            for i in (1, 2, 3):
                z_copy(w, planes[i], planes[1], 1 + i).wait_send()


def fused_layer(
    tokens, norm1_gain, weight_u, weight_v, scale_u, scale_v, mix_gain, spatial_weight,
    spatial_bias, weight_out, scale_out, norm2_gain, weight_up, scale_up, weight_down, scale_down,
):
    rows, fine = tokens.shape
    depth, width, hid = norm1_gain.shape[0], weight_u.shape[1], weight_up.shape[1]
    bf16, f32 = jnp.bfloat16, jnp.float32
    vmem = lambda shape, kind: pltpu.VMEM(shape, kind)
    dma = lambda *shape: pltpu.SemaphoreType.DMA(shape)
    row = lambda value: value[None, :]
    hbm = pl.BlockSpec(memory_space=pl.ANY)
    local = pl.BlockSpec(memory_space=pltpu.VMEM)
    return pl.pallas_call(
        fused_kernel,
        name="fused_layer",
        out_shape=jax.ShapeDtypeStruct((rows, fine), bf16),
        in_specs=[hbm] * 6 + [local] * 10,
        out_specs=local,
        scratch_shapes=[
            vmem((4, fine, fine), f32),
            vmem((depth, 2 * width), bf16),
            vmem((4, width, fine), bf16),
            vmem((2, depth, hid // 2), bf16),
            vmem((4, hid, fine), bf16),
            vmem((4, rows, fine), bf16),
            vmem((4, rows, fine), bf16),
            vmem((rows, depth), bf16),
            vmem((rows, hid), bf16),
            vmem((rows, width), f32),
            vmem((rows, width), f32),
            vmem((rows, width), bf16),
            vmem((rows, 128), f32),
            vmem((4, 8, rows), f32),
            vmem((4, 2, fine), f32),
            vmem((4, rows, fine), bf16),
            vmem((2, rows, fine), bf16),
            vmem((rows, fine), bf16),
            vmem((rows, fine), bf16),
            dma(6),
            dma(WAVES, 5), dma(WAVES, 4), dma(WAVES, 3), dma(WAVES, 4),
            dma(2, 3, CHUNKS), dma(2, 4, CHUNKS),
            dma(2, CHUNKS), dma(2, CHUNKS), dma(CHUNKS), dma(CHUNKS),
            dma(4, CHUNKS), dma(2, CHUNKS), dma(CHUNKS), dma(CHUNKS),
            dma(3), dma(4), dma(3), dma(4),
        ],
        compiler_params=pltpu.CompilerParams(
            collective_id=0, has_side_effects=True, vmem_limit_bytes=67043328
        ),
    )(
        tokens, weight_u, weight_v, weight_out, weight_up, weight_down,
        row(norm1_gain), row(scale_u), row(scale_v), row(mix_gain), spatial_weight, spatial_bias,
        row(scale_out), row(scale_down), row(norm2_gain), row(scale_up),
    )


def solution(mesh):
    placed = (
        P(("grp", "fs"), "tp"),
        P(),
        P("fs", "tp"),
        P("fs", "tp"),
        P("tp"),
        P("tp"),
        P("tp"),
        P(),
        P(),
        P("tp", "fs"),
        P("fs"),
        P(),
        P("fs", "tp"),
        P("tp"),
        P("tp", "fs"),
        P("fs"),
    )
    grp, fs, tp = mesh.shape["grp"], mesh.shape["fs"], mesh.shape["tp"]
    fused = grp == 2 and fs == 4 and tp == 4
    return jax.shard_map(
        fused_layer if fused else make(fs, tp),
        mesh=mesh,
        in_specs=placed,
        out_specs=P(("grp", "fs"), "tp"),
        check_vma=False,
    )
```

```python
import jax
import jax.numpy as jnp
from jax import lax
from jax.experimental import pallas as pl
from jax.experimental.pallas import tpu as pltpu
from jax.sharding import PartitionSpec as P

GM_W = 1024
GROUPS = 4
BLOCK = 128


def swap(value, axis, size, mask):
    return lax.ppermute(value, axis, [(k, k ^ mask) for k in range(size)])


def over_fs(piece, fs, relay, near_too):
    if fs != 4 or not relay:
        return [piece] + [swap(piece, "fs", fs, mask) for mask in range(1, fs)]
    far = swap(piece, "fs", 4, 2)
    near = swap(piece, "fs", 4, 1) if near_too else None
    middle = lax.ppermute(piece, "fs", [(1, 2), (2, 1)])
    relayed = lax.ppermute(far, "fs", [(1, 0), (2, 3)])
    me = lax.axis_index("fs")
    last = jnp.where((me == 1) | (me == 2), middle, relayed)
    return [piece, near, far, last]


def gather_weight(shard, cut_axis, fs, relay=False, whole_near=False):
    half = shard.shape[cut_axis] // 2
    group = lax.axis_index("grp")
    mine = lax.dynamic_slice_in_dim(shard, group * half, half, cut_axis)
    other = lax.dynamic_slice_in_dim(shard, (1 - group) * half, half, cut_axis)
    whole_near = whole_near and relay and fs == 4
    firsts = over_fs(mine, fs, relay, not whole_near)
    if whole_near:
        near = swap(jnp.concatenate([mine, other], axis=cut_axis), "fs", fs, 1)
        firsts[1], near_other = jnp.split(near, 2, axis=cut_axis)
    seconds = [other] + [
        near_other
        if whole_near and mask == 1
        else lax.ppermute(firsts[mask], "grp", [(0, 1), (1, 0)])
        for mask in range(1, fs)
    ]
    return firsts, seconds


def halves_swapped(value, axis):
    half = value.shape[axis] // 2
    group = lax.axis_index("grp")
    return jnp.concatenate(
        [
            lax.dynamic_slice_in_dim(value, group * half, half, axis),
            lax.dynamic_slice_in_dim(value, (1 - group) * half, half, axis),
        ],
        axis=axis,
    )


def gather_rows(piece, tp):
    blocks = [None] * tp
    blocks[0] = piece
    bit = tp // 2
    while bit:
        for at in range(tp):
            if blocks[at] is not None and not at & bit and blocks[at | bit] is None:
                blocks[at | bit] = "due"
        for at in range(tp):
            if isinstance(blocks[at], str):
                blocks[at] = swap(blocks[at ^ bit], "tp", tp, bit)
        bit //= 2
    return blocks


def normed_blocks(blocks, gain, fs, tp):
    feature_count = gain.shape[0]
    width, fine = feature_count // tp, feature_count // fs
    squares = sum(
        jnp.sum(jnp.square(block.astype(jnp.float32)), axis=1) for block in blocks
    )
    inverse = lax.rsqrt(squares / feature_count + 1e-06)[:, None]
    stacked = jnp.stack(blocks)
    me_fs, me_tp = lax.axis_index("fs"), lax.axis_index("tp")
    pieces = []
    for mask in range(fs):
        block = me_fs ^ mask
        first = block * fine
        whole = lax.dynamic_index_in_dim(stacked, (first // width) ^ me_tp, 0, keepdims=False)
        if fine != width:
            whole = lax.dynamic_slice_in_dim(whole, first % width, fine, 1)
        gain_piece = lax.dynamic_slice_in_dim(gain, first, fine, 0)
        pieces.append((whole.astype(jnp.float32) * inverse * gain_piece).astype(jnp.bfloat16))
    return jnp.concatenate(pieces, axis=1)


def scatter_sum(terms, fs, tp):
    stacked = jnp.stack(terms)
    ratio = fs // tp
    me_fs, me_tp = lax.axis_index("fs"), lax.axis_index("tp")
    sums = []
    for mask in range(tp):
        parts = [
            lax.dynamic_index_in_dim(
                stacked, ((me_tp ^ mask) * ratio + at) ^ me_fs, 0, keepdims=False
            )
            for at in range(ratio)
        ]
        sums.append(parts[0] if ratio == 1 else jnp.concatenate(parts, axis=1))
    bit = 1
    while bit < tp:
        kept = {}
        for at in range(tp):
            if sums[at] is not None and not at & bit:
                got = swap(sums[at | bit].astype(jnp.bfloat16), "tp", tp, bit)
                kept[at] = sums[at].astype(jnp.float32) + got.astype(jnp.float32)
        sums = [kept.get(at) for at in range(tp)]
        bit *= 2
    return sums[0]


def make(fs, tp):
    def layer(
        tokens,
        norm1_gain,
        weight_u,
        weight_v,
        scale_u,
        scale_v,
        mix_gain,
        spatial_weight,
        spatial_bias,
        weight_out,
        scale_out,
        norm2_gain,
        weight_up,
        scale_up,
        weight_down,
        scale_down,
    ):
        half = weight_u.shape[1] // 2
        token_blocks = gather_rows(tokens, tp)
        both = jnp.stack([weight_u, weight_v], axis=1).astype(jnp.bfloat16)
        both_mine, both_other = gather_weight(both, 2, fs)
        scales = jnp.stack([scale_out, scale_down])
        all_scales = [scales] + [swap(scales, "fs", fs, mask) for mask in range(1, fs)]
        out_mine, out_other = gather_weight(weight_out.astype(jnp.bfloat16), 0, fs)
        up_mine, up_other = gather_weight(weight_up.astype(jnp.bfloat16), 1, fs, relay=True)
        down_mine, down_other = gather_weight(weight_down.astype(jnp.bfloat16), 0, fs, relay=True, whole_near=True)

        normed_in = normed_blocks(token_blocks, norm1_gain, fs, tp)
        full_u = jnp.concatenate(
            [jnp.concatenate([a[:, 0], b[:, 0]], axis=1) for a, b in zip(both_mine, both_other)]
        )
        full_v = jnp.concatenate(
            [jnp.concatenate([a[:, 1], b[:, 1]], axis=1) for a, b in zip(both_mine, both_other)]
        )
        pre_v = jnp.dot(normed_in, full_v, preferred_element_type=jnp.float32)
        pre_u = jnp.dot(normed_in, full_u, preferred_element_type=jnp.float32)
        act_v = jax.nn.gelu(pre_v * halves_swapped(scale_v, 0))
        gate_u = jax.nn.gelu(pre_u * halves_swapped(scale_u, 0))
        local_width = 2 * half
        row_sums, row_squares = lax.psum(
            (jnp.sum(act_v, axis=1), jnp.sum(act_v * act_v, axis=1)), "tp"
        )
        row_mean = (row_sums / GM_W)[:, None]
        square = (row_squares / GM_W)[:, None]
        v_norm = (
            (act_v - row_mean)
            * lax.rsqrt(square - row_mean * row_mean + 1e-06)
            * halves_swapped(mix_gain, 0)
        ).astype(jnp.bfloat16)
        group_index = lax.axis_index("tp") * local_width // (GM_W // GROUPS)
        lower_mask = jnp.tril(jnp.ones((BLOCK, BLOCK), jnp.float32))
        spatial_mask = (
            lax.dynamic_index_in_dim(spatial_weight, group_index, 0, keepdims=False) * lower_mask
        ).astype(jnp.bfloat16)
        block_bias = lax.dynamic_index_in_dim(spatial_bias, group_index, 0, keepdims=False)
        blocks = v_norm.reshape(-1, BLOCK, local_width)
        mixed = jnp.einsum("ts,nsc->ntc", spatial_mask, blocks, preferred_element_type=jnp.float32)
        mixed = mixed + block_bias[None, :, None]
        gated = (gate_u * mixed.reshape(-1, local_width)).astype(jnp.bfloat16)

        terms = []
        for a, b, scale in zip(out_mine, out_other, all_scales):
            product = jnp.dot(gated, jnp.concatenate([a, b]), preferred_element_type=jnp.float32)
            terms.append((product * scale[0]).astype(jnp.bfloat16))
        mixer_sum = scatter_sum(terms, fs, tp)
        residual = (tokens.astype(jnp.float32) + mixer_sum).astype(jnp.bfloat16)

        normed_mid = normed_blocks(gather_rows(residual, tp), norm2_gain, fs, tp)
        full_up = jnp.concatenate(
            [jnp.concatenate([a, b], axis=1) for a, b in zip(up_mine, up_other)]
        )
        pre_up = jnp.dot(normed_mid, full_up, preferred_element_type=jnp.float32)
        hidden = jnp.square(jax.nn.relu(pre_up * halves_swapped(scale_up, 0))).astype(jnp.bfloat16)
        terms = []
        for a, b, scale in zip(down_mine, down_other, all_scales):
            product = jnp.dot(hidden, jnp.concatenate([a, b]), preferred_element_type=jnp.float32)
            terms.append((product * scale[1]).astype(jnp.bfloat16))
        channel_sum = scatter_sum(terms, fs, tp)
        return (residual.astype(jnp.float32) + channel_sum).astype(jnp.bfloat16)

    return layer


MESH = pl.DeviceIdType.MESH
WAVES = 6
CHUNKS = 4
STEP = 64


def rows_of(first, size, unit):
    return pl.ds(pl.multiple_of(first, unit), size)


def row_loop(first, count, step, body):
    def at(i, carry):
        body(rows_of(first + i * step, step, step))
        return carry

    lax.fori_loop(0, count // step, at, 0)


def matmul(a, b):
    return jnp.dot(a, b, preferred_element_type=jnp.float32)


def fused_kernel(
    tokens, weight_u, weight_v, weight_out, weight_up, weight_down,
    gain1, scale_u, scale_v, mix_gain, spatial_weight, spatial_bias,
    scale_out, scale_down, gain2, scale_up,
    result,
    stage, g_both, g_out, g_up, g_down, tok, mid, mid_end, normed, hidden, hidden_end,
    act_v, gate_u, gated, stat, stat_rows, scales, terms, core_in, core_end, x_out, x_in, x_end,
    load_sem, zs, zr, ys, yr, zos, zor, gs, gr, cs, cr, xs, xr, cs2, cr2, xs2, xr2,
    cs3, cr3, xs3, xr3, es, er, ps, pr, sts, strv, scs, scr,
):
    y, z, t = lax.axis_index("grp"), lax.axis_index("fs"), lax.axis_index("tp")
    other_y = 1 - y
    upper = z // 2
    planes = (z, 1 - z + 4 * upper, 2 - upper, 3 - 3 * upper)
    is_mid = (z == 1) | (z == 2)
    is_end = jnp.logical_not(is_mid)
    terms_end = tok
    inner = (t == 1) | (t == 2)
    outer = jnp.logical_not(inner)
    t1 = t + 1 - 2 * (t % 2)
    t2 = (t + 2) % 4
    t3 = (t1 + 2) % 4
    rows, fine = tokens.shape
    chunk = rows // CHUNKS
    width = weight_u.shape[1]
    hid = weight_up.shape[1]
    hhalf = hid // 2
    feature_count = gain1.shape[1]
    sends = []

    def remote(source, target, send, recv, **where):
        return pltpu.make_async_remote_copy(
            src_ref=source, dst_ref=target, send_sem=send, recv_sem=recv,
            device_id=where, device_id_type=MESH,
        )

    barrier = pltpu.get_barrier_semaphore()
    for p in planes[1:]:
        pl.semaphore_signal(barrier, inc=1, device_id={"fs": p}, device_id_type=MESH)
    pl.semaphore_signal(barrier, inc=1, device_id={"grp": other_y}, device_id_type=MESH)
    for u in (t1, t2, t3):
        pl.semaphore_signal(barrier, inc=1, device_id={"tp": u}, device_id_type=MESH)

    def load(source, slot, part=None):
        target = stage.at[slot] if part is None else part
        return pltpu.make_async_copy(source, target, load_sem.at[slot])

    half_w = width
    load_u = load(weight_u, 0, stage.at[0, :, pl.ds(0, half_w)])
    load_v = pltpu.make_async_copy(weight_v, stage.at[0, :, pl.ds(half_w, half_w)], load_sem.at[4])
    load_out = load(weight_out, 1, stage.at[1, pl.ds(0, width), :])
    load_tok = pltpu.make_async_copy(tokens, tok.at[t], load_sem.at[5])

    def load_up(j, slot):
        return load(weight_up.at[:, pl.ds(j * fine, fine)], slot)

    def load_down(j, slot):
        return load(weight_down.at[pl.ds(j * fine, fine), :], slot)

    load_u.start()
    load_v.start()
    load_out.start()
    load_up(0, 2).start()
    load_up(1, 3).start()
    load_tok.start()
    scales[z] = jnp.concatenate([scale_out[...], scale_down[...]], axis=0)

    pl.semaphore_wait(barrier, 7)

    def gather_copies(which, buffer, own_source, r):
        part = pl.ds(r * chunk, chunk)
        to_x = remote(own_source.at[part], buffer.at[t, part], gs.at[which, 0, r], gr.at[which, t, r], tp=t2)
        to_core = remote(own_source.at[part], buffer.at[t, part], gs.at[which, 1, r], gr.at[which, t, r], tp=t1)
        return to_x, to_core

    def gather_start(which, buffer, own_source, r):
        for copy in gather_copies(which, buffer, own_source, r):
            copy.start()
            sends.append(copy)

    def gather_await(which, buffer, block, r):
        part = pl.ds(r * chunk, chunk)
        remote(buffer.at[block, part], buffer.at[block, part], gs.at[which, 2, r], gr.at[which, block, r], tp=t1).wait_recv()

    def relay_copy(which, buffer, r):
        part = pl.ds(r * chunk, chunk)
        return remote(buffer.at[t2, part], buffer.at[t2, part], gs.at[which, 2, r], gr.at[which, t2, r], tp=t1)

    def gather_relay(which, buffer, r, listed=True):
        gather_await(which, buffer, t2, r)
        copy = relay_copy(which, buffer, r)
        copy.start()
        if listed:
            sends.append(copy)

    def piece(w, p, h):
        if w == 0:
            size = fine // 2
            return g_both.at[rows_of(p * fine + h * size, size, size), :]
        if w == 1:
            size = width // 2
            return g_out.at[p, rows_of(h * size, size, size), :]
        if w < 4:
            size = fine // 2
            return g_up.at[h, rows_of(p * fine + (w - 2) * size, size, size), :]
        size = hhalf // 2
        return g_down.at[p, rows_of(h * hhalf + (w - 4) * size, size, size), :]

    def z_copy(w, p, to, slot):
        return remote(piece(w, p, y), piece(w, p, y), zs.at[w, slot], zr.at[w, p], fs=to)

    def y_copy(w, i, h):
        p = planes[i]
        return remote(piece(w, p, h), piece(w, p, h), ys.at[w, i - 1], yr.at[w, p], grp=other_y)

    def own(w):
        z_copy(w, z, planes[1], 0).start()

        @pl.when(is_mid)
        def _():
            z_copy(w, z, planes[2], 1).start()

    def arrive(w, i):
        p = planes[i]
        z_copy(w, p, planes[1], 1 + i).wait_recv()

        @pl.when(is_mid)
        def _():
            z_copy(w, p, planes[2] if i == 1 else planes[1], 1 + i).start()

        y_copy(w, i, y).start()

    def arrive_y(w, i):
        y_copy(w, i, other_y).wait_recv()

    def arrive_all_y(w):
        for i in (1, 2, 3):
            arrive_y(w, i)

    def other_half(w, p):
        return remote(piece(w, p, other_y), piece(w, p, other_y), zos.at[w], zor.at[w], fs=planes[1])

    def own_end(w, first):
        @pl.when(is_end)
        def _():
            (z_copy(w, z, planes[1], 0) if first else other_half(w, z)).start()

    def own_mid(w):
        @pl.when(is_mid)
        def _():
            z_copy(w, z, planes[2], 1).start()

    def pass_on(w, i):
        @pl.when(is_mid)
        def _():
            p = planes[i]
            z_copy(w, p, planes[1], 1 + i).wait_recv()
            if i == 1:
                z_copy(w, p, planes[2], 2).start()
            else:
                y_copy(w, i, y).start()

    for r in range(CHUNKS):
        gather_start(0, tok, tokens, r)

    def cast_to(slot, count, store):
        row_loop(0, count, STEP, lambda part: store(part, stage[slot, part, :].astype(jnp.bfloat16)))

    def at_offset(part, base):
        return rows_of(part.start + base, part.size, part.size)

    load_u.wait()
    load_v.wait()

    def store_both(part, value):
        g_both[at_offset(part, z * fine), :] = value

    cast_to(0, fine, store_both)
    load_up(2, 0).start()
    load_out.wait()

    def store_out(part, value):
        g_out[z, part, :] = value

    own(0)
    cast_to(1, width, store_out)
    load_up(3, 1).start()
    for i in (1, 2, 3):
        copy = remote(scales.at[z], scales.at[z], scs.at[i - 1], scr.at[z], fs=planes[i])
        copy.start()
        sends.append(copy)

    def cast_up(j, slot):
        load_up(j, slot).wait()
        cols = pl.ds((j % 2) * fine, fine)

        def store(part, value):
            g_up[j // 2, at_offset(part, z * fine), cols] = value

        cast_to(slot, fine, store)

    def cast_down(j, slot):
        load_down(j, slot).wait()

        def store(part, value):
            g_down[z, at_offset(part, j * fine), :] = value

        cast_to(slot, fine, store)

    cast_up(0, 2)
    load_down(0, 2).start()
    cast_up(1, 3)
    load_down(1, 3).start()
    arrive(0, 1)
    own(1)
    cast_up(2, 0)
    load_down(2, 0).start()
    cast_up(3, 1)
    load_down(3, 1).start()
    own_end(2, True)
    own_end(3, True)
    own_mid(2)
    arrive(0, 2)
    gather_relay(0, tok, 0)
    arrive(0, 3)
    gather_relay(0, tok, 1)
    cast_down(0, 2)
    cast_down(1, 3)
    cast_down(2, 0)
    cast_down(3, 1)
    gather_relay(0, tok, 2)
    arrive(1, 1)
    arrive(1, 2)
    own_end(2, False)
    own_end(3, False)
    load_tok.wait()

    def norm_rows(buffer, gain, first, count):
        def body(part):
            total = jnp.zeros((part.size, 1), jnp.float32)
            for b in range(4):
                value = buffer[b, part, :].astype(jnp.float32)
                total = total + jnp.sum(value * value, axis=1, keepdims=True)
            inverse = lax.rsqrt(total / feature_count + 1e-06)
            for b in range(4):
                value = buffer[b, part, :].astype(jnp.float32)
                cols = pl.ds(b * fine, fine)
                normed[part, cols] = (value * inverse * gain[:, cols]).astype(jnp.bfloat16)

        row_loop(first, count, 32, body)

    def norm_chunk(which, buffer, gain, r):
        gather_await(which, buffer, t1, r)
        gather_await(which, buffer, t3, r)
        norm_rows(buffer, gain, r * chunk, chunk)

    for r in range(CHUNKS):
        if r == CHUNKS - 1:
            gather_relay(0, tok, r)
        norm_chunk(0, tok, gain1, r)

    own_mid(3)
    arrive_all_y(0)

    lane = lax.broadcasted_iota(jnp.int32, (chunk, 128), 1)

    def v_chunk(part):
        value = jax.nn.gelu(matmul(normed[part, :], g_both[:, width:]) * scale_v[...])
        act_v[part, :] = value
        total = jnp.sum(value, axis=1, keepdims=True)
        square = jnp.sum(value * value, axis=1, keepdims=True)
        stat[part, :] = jnp.where(lane == 0, total, jnp.where(lane == 1, square, 0.0))

    row_loop(0, rows, chunk, v_chunk)
    stat_rows[0] = stat[...].T[0:8]

    def stat_copy(k, u):
        return remote(stat_rows.at[0], stat_rows.at[k], sts.at[k - 1], strv.at[k], tp=u)

    def u_chunk(part):
        gate_u[part, :] = jax.nn.gelu(matmul(normed[part, :], g_both[:, :width]) * scale_u[...])

    for k, u in ((1, t1), (2, t2), (3, t3)):
        copy = stat_copy(k, u)
        copy.start()
        sends.append(copy)
    row_loop(0, rows, chunk, u_chunk)
    arrive(1, 3)
    for k, u in ((1, t1), (2, t2), (3, t3)):
        stat_copy(k, u).wait_recv()
    totals = stat_rows[0] + stat_rows[1] + stat_rows[2] + stat_rows[3]
    stat[...] = jnp.concatenate([totals, jnp.zeros((120, rows), jnp.float32)], axis=0).T

    down_at = lax.broadcasted_iota(jnp.int32, (BLOCK, BLOCK), 0)
    along = lax.broadcasted_iota(jnp.int32, (BLOCK, BLOCK), 1)
    mask = jnp.where(along <= down_at, spatial_weight[t], 0.0).astype(jnp.bfloat16)
    bias_row = spatial_bias[pl.ds(t, 1), :]
    bias = jnp.sum(jnp.where(along == down_at, bias_row, 0.0), axis=1, keepdims=True)

    def mix_block(part):
        mean = stat[part, 0:1] / GM_W
        square = stat[part, 1:2] / GM_W
        v_norm = (act_v[part, :] - mean) * lax.rsqrt(square - mean * mean + 1e-06) * mix_gain[...]
        mixed = matmul(mask, v_norm.astype(jnp.bfloat16)) + bias
        gated[part, :] = (gate_u[part, :] * mixed).astype(jnp.bfloat16)

    row_loop(0, rows, BLOCK, mix_block)
    pass_on(2, 1)
    own_end(4, True)
    arrive_all_y(1)
    for i in (1, 2, 3):
        remote(scales.at[planes[i]], scales.at[planes[i]], scs.at[i - 1], scr.at[planes[i]], fs=planes[i]).wait_recv()

    def core_copy(k, block, r):
        part = pl.ds(r * chunk, chunk)
        return remote(terms.at[block, part], core_in.at[k, part], cs.at[k, r], cr.at[k, r], tp=t1)

    def x_copy(send, recv, r):
        part = pl.ds(r * chunk, chunk)
        return remote(x_out.at[part], x_in.at[part], send.at[r], recv.at[r], tp=t2)

    def end_copy(r):
        part = pl.ds(r * chunk, chunk)
        return remote(mid.at[t, part], mid_end.at[t, part], gs.at[1, 0, r], gr.at[2, t, r], fs=planes[1])

    pass_on(2, 2)
    mix_sends = []
    for r in range(CHUNKS):
        part = pl.ds(r * chunk, chunk)
        for j in range(4):
            product = matmul(gated[part, :], g_out[j])
            terms[j, part, :] = (product * scales[j, 0:1, :]).astype(jnp.bfloat16)
        for k, block in ((0, t1), (1, t3)):
            copy = core_copy(k, block, r)
            copy.start()
            mix_sends.append(copy)

    def pair_out(block, slot, r):
        def body(part):
            both = terms[block, part, :].astype(jnp.float32) + core_in[slot, part, :].astype(jnp.float32)
            x_out[part, :] = both.astype(jnp.bfloat16)

        row_loop(r * chunk, chunk, STEP, body)

    for r in range(CHUNKS):
        core_copy(0, t1, r).wait_recv()
        core_copy(1, t3, r).wait_recv()
        pair_out(t2, 1, r)
        copy = x_copy(xs, xr, r)
        copy.start()
        mix_sends.append(copy)
    pass_on(3, 1)
    pass_on(3, 2)
    own_mid(4)

    for r in range(CHUNKS):
        x_copy(xs, xr, r).wait_recv()

        def residual_rows(part):
            total = terms[t, part, :].astype(jnp.float32) + core_in[0, part, :].astype(jnp.float32)
            total = total + x_in[part, :].astype(jnp.float32)
            mid[t, part, :] = (tok[t, part, :].astype(jnp.float32) + total).astype(jnp.bfloat16)

        row_loop(r * chunk, chunk, STEP, residual_rows)

        @pl.when(is_mid)
        def _():
            for copy in gather_copies(1, mid, mid.at[t], r):
                copy.start()

        @pl.when(is_end)
        def _():
            end_copy(r).start()

        if r == 2:
            pass_on(2, 3)

    for copy in sends + mix_sends:
        copy.wait_send()

    tile = min(hhalf, fine)

    def up_half(target, h, first=0, count=rows):
        def body(part):
            for n in range(hhalf // tile):
                cols = pl.ds(n * tile, tile)
                place = rows_of(h * hhalf + n * tile, tile, 128)
                value = matmul(normed[part, :], g_up[h, :, cols]) * scale_up[:, place]
                value = jnp.maximum(value, 0.0)
                target[part, place] = (value * value).astype(jnp.bfloat16)

        row_loop(first, count, chunk, body)

    sets = {
        True: (hidden, terms, core_in, cs2, cr2),
        False: (hidden_end, terms_end, core_end, cs3, cr3),
    }

    def chan_core(near, i, r):
        _, out, into, send, recv = sets[near]
        j = planes[i]
        part = rows_of(r * chunk, chunk, chunk)
        return remote(out.at[j, part], into.at[j // 2, part], send.at[i, r], recv.at[j // 2, r], tp=t1)

    def end_x_copy(slot, r):
        part = pl.ds(r * chunk, chunk)
        return remote(core_end.at[slot, part], x_end.at[part], xs3.at[r], xr3.at[r], tp=t2)

    def pair_copy(slot, r):
        part = pl.ds(r * chunk, chunk)
        return remote(core_end.at[slot, part], core_in.at[slot, part], ps.at[r], pr.at[r], fs=planes[1])

    def end_swap(slot, r):
        part = pl.ds(r * chunk, chunk)
        return remote(core_in.at[slot, part], x_in.at[part], xs2.at[r], xr2.at[r], tp=t2)

    def back_copy(r):
        part = pl.ds(r * chunk, chunk)
        return remote(x_end.at[part], x_in.at[part], es.at[r], er.at[r], fs=planes[1])

    def down_dots(near, i):
        source, out = sets[near][:2]
        j = planes[i]
        mine = (j % 2) == (t % 2)

        def one(r, carry):
            part = rows_of(r * chunk, chunk, chunk)
            product = matmul(source[part, :], g_down[j])
            out[j, part, :] = (product * scales[j, 1:2, :]).astype(jnp.bfloat16)

            @pl.when(jnp.logical_not(mine))
            def _():
                chan_core(near, i, r).start()

            return carry

        lax.fori_loop(0, CHUNKS, one, 0)

    def pair_up(near, i):
        j = planes[i]
        slot = j // 2

        @pl.when((j % 2) == (t % 2))
        def _():
            for r in range(CHUNKS):
                chan_core(near, i, r).wait_recv()
                if near:
                    @pl.when(j != t)
                    def _():
                        pair_out(j, slot, r)
                        x_copy(xs2, xr2, r).start()
                else:
                    def body(part):
                        both = tok[j, part, :].astype(jnp.float32) + core_end[slot, part, :].astype(jnp.float32)
                        core_end[slot, part, :] = both.astype(jnp.bfloat16)

                    if i in (0, 2):
                        row_loop(r * chunk, chunk, STEP, body)
                        pair_copy(slot, r).start()
                    else:
                        @pl.when(j != t)
                        def _():
                            row_loop(r * chunk, chunk, STEP, body)
                            end_x_copy(slot, r).start()

    def finish_end(i):
        @pl.when(planes[i] == t)
        def _():
            for r in range(CHUNKS):
                end_x_copy(t2 // 2, r).wait_recv()

                def end_rows(part):
                    total = tok[t, part, :].astype(jnp.float32) + core_end[t // 2, part, :].astype(jnp.float32)
                    total = total + x_end[part, :].astype(jnp.float32)
                    x_end[part, :] = (mid_end[t, part, :].astype(jnp.float32) + total).astype(jnp.bfloat16)

                row_loop(r * chunk, chunk, STEP, end_rows)
                back_copy(r).start()

    @pl.when(is_mid)
    def _():
        own_mid(5)
        gather_relay(1, mid, 0, False)
        norm_chunk(1, mid, gain2, 0)
        pass_on(3, 3)
        gather_relay(1, mid, 1, False)
        norm_chunk(1, mid, gain2, 1)
        other_half(2, planes[1]).wait_recv()
        other_half(3, planes[1]).wait_recv()
        up_half(hidden, y, 0, 2 * chunk)
        gather_relay(1, mid, 2, False)
        norm_chunk(1, mid, gain2, 2)
        up_half(hidden, y, 2 * chunk, chunk)
        pass_on(4, 1)
        for r in range(CHUNKS):
            gather_await(2, mid_end, t, r)
            for copy in gather_copies(2, mid_end, mid_end.at[t], r):
                copy.start()
        pass_on(4, 2)
        pass_on(5, 2)
        gather_relay(1, mid, 3, False)
        norm_chunk(1, mid, gain2, 3)
        up_half(hidden, y, 3 * chunk, chunk)
        for w in (2, 3):
            for i in (2, 3):
                arrive_y(w, i)
        up_half(hidden, other_y)
        pass_on(4, 3)
        pass_on(5, 1)

        def end_chunk(r):
            norm_chunk(2, mid_end, gain2, r)
            for h in (0, 1):
                up_half(hidden_end, h, r * chunk, chunk)

        gather_relay(2, mid_end, 0, False)
        gather_relay(2, mid_end, 1, False)
        end_chunk(0)
        gather_relay(2, mid_end, 2, False)
        end_chunk(1)
        down_dots(True, 0)
        gather_relay(2, mid_end, 3, False)
        end_chunk(2)
        pair_up(True, 0)
        pass_on(5, 3)
        end_chunk(3)
        for w in (4, 5):
            arrive_y(w, 2)
        down_dots(False, 0)
        down_dots(False, 2)
        pair_up(False, 0)
        down_dots(True, 2)
        for w in (4, 5):
            other_half(w, planes[1]).wait_recv()
        pair_up(False, 2)
        down_dots(False, 1)
        pair_up(True, 2)
        for w in (4, 5):
            arrive_y(w, 3)
        down_dots(False, 3)
        pair_up(False, 1)
        down_dots(True, 1)
        pair_up(False, 3)
        down_dots(True, 3)
        pair_up(True, 1)
        pair_up(True, 3)
        for i in (1, 3):
            finish_end(i)
        for r in range(CHUNKS):
            x_copy(xs2, xr2, r).wait_recv()

            def result_rows(part):
                total = terms[t, part, :].astype(jnp.float32) + core_in[t // 2, part, :].astype(jnp.float32)
                total = total + x_in[part, :].astype(jnp.float32)
                result[part, :] = (mid[t, part, :].astype(jnp.float32) + total).astype(jnp.bfloat16)

            row_loop(r * chunk, chunk, STEP, result_rows)

    @pl.when(is_end)
    def _():
        z_copy(5, z, planes[1], 0).start()
        z_copy(5, z, planes[1], 0).wait_send()
        for w in (4, 5):
            other_half(w, z).start()
        near_slot = 1 - t % 2
        for r in range(CHUNKS):
            pair_copy(near_slot, r).wait_recv()

            @pl.when(outer)
            def _():
                end_swap(near_slot, r).start()

        @pl.when(inner)
        def _():
            for r in range(CHUNKS):
                end_swap(near_slot, r).wait_recv()

                def sum_rows(part):
                    total = core_in[near_slot, part, :].astype(jnp.float32) + x_in[part, :].astype(jnp.float32)
                    result[part, :] = (mid[t, part, :].astype(jnp.float32) + total).astype(jnp.bfloat16)

                row_loop(r * chunk, chunk, STEP, sum_rows)

        @pl.when(outer)
        def _():
            for r in range(CHUNKS):
                back_copy(r).wait_recv()

                def take_rows(part):
                    result[part, :] = x_in[part, :]

                row_loop(r * chunk, chunk, STEP, take_rows)
                end_swap(near_slot, r).wait_send()

    for w in (0, 1):
        z_copy(w, z, planes[1], 0).wait_send()
        for i in (1, 2, 3):
            y_copy(w, i, y).wait_send()

    @pl.when(is_end)
    def _():
        for w in range(2, WAVES):
            if w < 5:
                z_copy(w, z, planes[1], 0).wait_send()
            other_half(w, z).wait_send()
        for r in range(CHUNKS):
            end_copy(r).wait_send()

    @pl.when(is_mid)
    def _():
        for w in (0, 1):
            z_copy(w, z, planes[2], 1).wait_send()
            for i in (1, 2, 3):
                z_copy(w, planes[i], planes[1], 1 + i).wait_send()
        for w in range(2, WAVES):
            z_copy(w, z, planes[2], 1).wait_send()
            z_copy(w, planes[1], planes[2], 2).wait_send()
            for i in (2, 3):
                y_copy(w, i, y).wait_send()
        for r in range(CHUNKS):
            x_copy(xs2, xr2, r).wait_send()
            for which, buffer in ((1, mid), (2, mid_end)):
                for copy in gather_copies(which, buffer, buffer.at[t], r):
                    copy.wait_send()
                relay_copy(which, buffer, r).wait_send()
            pair_copy(1 - t % 2, r).wait_send()

            @pl.when(inner)
            def _():
                end_x_copy(t2 // 2, r).wait_send()

            @pl.when(outer)
            def _():
                back_copy(r).wait_send()
        for i in range(4):
            @pl.when((planes[i] % 2) != (t % 2))
            def _():
                for r in range(CHUNKS):
                    chan_core(True, i, r).wait_send()
                    chan_core(False, i, r).wait_send()


def fused_layer(
    tokens, norm1_gain, weight_u, weight_v, scale_u, scale_v, mix_gain, spatial_weight,
    spatial_bias, weight_out, scale_out, norm2_gain, weight_up, scale_up, weight_down, scale_down,
):
    rows, fine = tokens.shape
    depth, width, hid = norm1_gain.shape[0], weight_u.shape[1], weight_up.shape[1]
    bf16, f32 = jnp.bfloat16, jnp.float32
    vmem = lambda shape, kind: pltpu.VMEM(shape, kind)
    dma = lambda *shape: pltpu.SemaphoreType.DMA(shape)
    row = lambda value: value[None, :]
    hbm = pl.BlockSpec(memory_space=pl.ANY)
    local = pl.BlockSpec(memory_space=pltpu.VMEM)
    return pl.pallas_call(
        fused_kernel,
        name="fused_layer",
        out_shape=jax.ShapeDtypeStruct((rows, fine), bf16),
        in_specs=[hbm] * 6 + [local] * 10,
        out_specs=local,
        scratch_shapes=[
            vmem((4, fine, fine), f32),
            vmem((depth, 2 * width), bf16),
            vmem((4, width, fine), bf16),
            vmem((2, depth, hid // 2), bf16),
            vmem((4, hid, fine), bf16),
            vmem((4, rows, fine), bf16),
            vmem((4, rows, fine), bf16),
            vmem((4, rows, fine), bf16),
            vmem((rows, depth), bf16),
            vmem((rows, hid), bf16),
            vmem((rows, hid), bf16),
            vmem((rows, width), f32),
            vmem((rows, width), f32),
            vmem((rows, width), bf16),
            vmem((rows, 128), f32),
            vmem((4, 8, rows), f32),
            vmem((4, 2, fine), f32),
            vmem((4, rows, fine), bf16),
            vmem((2, rows, fine), bf16),
            vmem((2, rows, fine), bf16),
            vmem((rows, fine), bf16),
            vmem((rows, fine), bf16),
            vmem((rows, fine), bf16),
            dma(6),
            dma(WAVES, 5), dma(WAVES, 4), dma(WAVES, 3), dma(WAVES, 4), dma(WAVES), dma(WAVES),
            dma(3, 3, CHUNKS), dma(3, 4, CHUNKS),
            dma(2, CHUNKS), dma(2, CHUNKS), dma(CHUNKS), dma(CHUNKS),
            dma(4, CHUNKS), dma(2, CHUNKS), dma(CHUNKS), dma(CHUNKS),
            dma(4, CHUNKS), dma(2, CHUNKS), dma(CHUNKS), dma(CHUNKS), dma(CHUNKS), dma(CHUNKS), dma(CHUNKS), dma(CHUNKS),
            dma(3), dma(4), dma(3), dma(4),
        ],
        compiler_params=pltpu.CompilerParams(
            collective_id=0, has_side_effects=True, vmem_limit_bytes=67043328
        ),
    )(
        tokens, weight_u, weight_v, weight_out, weight_up, weight_down,
        row(norm1_gain), row(scale_u), row(scale_v), row(mix_gain), spatial_weight, spatial_bias,
        row(scale_out), row(scale_down), row(norm2_gain), row(scale_up),
    )


def solution(mesh):
    placed = (
        P(("grp", "fs"), "tp"),
        P(),
        P("fs", "tp"),
        P("fs", "tp"),
        P("tp"),
        P("tp"),
        P("tp"),
        P(),
        P(),
        P("tp", "fs"),
        P("fs"),
        P(),
        P("fs", "tp"),
        P("tp"),
        P("tp", "fs"),
        P("fs"),
    )
    grp, fs, tp = mesh.shape["grp"], mesh.shape["fs"], mesh.shape["tp"]
    fused = grp == 2 and fs == 4 and tp == 4
    return jax.shard_map(
        fused_layer if fused else make(fs, tp),
        mesh=mesh,
        in_specs=placed,
        out_specs=P(("grp", "fs"), "tp"),
        check_vma=False,
    )
```

```python
import jax
import jax.numpy as jnp
from jax import lax
from jax.experimental import pallas as pl
from jax.experimental.pallas import tpu as pltpu
from jax.sharding import PartitionSpec as P

GM_W = 1024
GROUPS = 4
BLOCK = 128


def swap(value, axis, size, mask):
    return lax.ppermute(value, axis, [(k, k ^ mask) for k in range(size)])


def over_fs(piece, fs, relay, near_too):
    if fs != 4 or not relay:
        return [piece] + [swap(piece, "fs", fs, mask) for mask in range(1, fs)]
    far = swap(piece, "fs", 4, 2)
    near = swap(piece, "fs", 4, 1) if near_too else None
    middle = lax.ppermute(piece, "fs", [(1, 2), (2, 1)])
    relayed = lax.ppermute(far, "fs", [(1, 0), (2, 3)])
    me = lax.axis_index("fs")
    last = jnp.where((me == 1) | (me == 2), middle, relayed)
    return [piece, near, far, last]


def gather_weight(shard, cut_axis, fs, relay=False, whole_near=False):
    half = shard.shape[cut_axis] // 2
    group = lax.axis_index("grp")
    mine = lax.dynamic_slice_in_dim(shard, group * half, half, cut_axis)
    other = lax.dynamic_slice_in_dim(shard, (1 - group) * half, half, cut_axis)
    whole_near = whole_near and relay and fs == 4
    firsts = over_fs(mine, fs, relay, not whole_near)
    if whole_near:
        near = swap(jnp.concatenate([mine, other], axis=cut_axis), "fs", fs, 1)
        firsts[1], near_other = jnp.split(near, 2, axis=cut_axis)
    seconds = [other] + [
        near_other
        if whole_near and mask == 1
        else lax.ppermute(firsts[mask], "grp", [(0, 1), (1, 0)])
        for mask in range(1, fs)
    ]
    return firsts, seconds


def halves_swapped(value, axis):
    half = value.shape[axis] // 2
    group = lax.axis_index("grp")
    return jnp.concatenate(
        [
            lax.dynamic_slice_in_dim(value, group * half, half, axis),
            lax.dynamic_slice_in_dim(value, (1 - group) * half, half, axis),
        ],
        axis=axis,
    )


def gather_rows(piece, tp):
    blocks = [None] * tp
    blocks[0] = piece
    bit = tp // 2
    while bit:
        for at in range(tp):
            if blocks[at] is not None and not at & bit and blocks[at | bit] is None:
                blocks[at | bit] = "due"
        for at in range(tp):
            if isinstance(blocks[at], str):
                blocks[at] = swap(blocks[at ^ bit], "tp", tp, bit)
        bit //= 2
    return blocks


def normed_blocks(blocks, gain, fs, tp):
    feature_count = gain.shape[0]
    width, fine = feature_count // tp, feature_count // fs
    squares = sum(
        jnp.sum(jnp.square(block.astype(jnp.float32)), axis=1) for block in blocks
    )
    inverse = lax.rsqrt(squares / feature_count + 1e-06)[:, None]
    stacked = jnp.stack(blocks)
    me_fs, me_tp = lax.axis_index("fs"), lax.axis_index("tp")
    pieces = []
    for mask in range(fs):
        block = me_fs ^ mask
        first = block * fine
        whole = lax.dynamic_index_in_dim(stacked, (first // width) ^ me_tp, 0, keepdims=False)
        if fine != width:
            whole = lax.dynamic_slice_in_dim(whole, first % width, fine, 1)
        gain_piece = lax.dynamic_slice_in_dim(gain, first, fine, 0)
        pieces.append((whole.astype(jnp.float32) * inverse * gain_piece).astype(jnp.bfloat16))
    return jnp.concatenate(pieces, axis=1)


def scatter_sum(terms, fs, tp):
    stacked = jnp.stack(terms)
    ratio = fs // tp
    me_fs, me_tp = lax.axis_index("fs"), lax.axis_index("tp")
    sums = []
    for mask in range(tp):
        parts = [
            lax.dynamic_index_in_dim(
                stacked, ((me_tp ^ mask) * ratio + at) ^ me_fs, 0, keepdims=False
            )
            for at in range(ratio)
        ]
        sums.append(parts[0] if ratio == 1 else jnp.concatenate(parts, axis=1))
    bit = 1
    while bit < tp:
        kept = {}
        for at in range(tp):
            if sums[at] is not None and not at & bit:
                got = swap(sums[at | bit].astype(jnp.bfloat16), "tp", tp, bit)
                kept[at] = sums[at].astype(jnp.float32) + got.astype(jnp.float32)
        sums = [kept.get(at) for at in range(tp)]
        bit *= 2
    return sums[0]


def make(fs, tp):
    def layer(
        tokens,
        norm1_gain,
        weight_u,
        weight_v,
        scale_u,
        scale_v,
        mix_gain,
        spatial_weight,
        spatial_bias,
        weight_out,
        scale_out,
        norm2_gain,
        weight_up,
        scale_up,
        weight_down,
        scale_down,
    ):
        half = weight_u.shape[1] // 2
        token_blocks = gather_rows(tokens, tp)
        both = jnp.stack([weight_u, weight_v], axis=1).astype(jnp.bfloat16)
        both_mine, both_other = gather_weight(both, 2, fs)
        scales = jnp.stack([scale_out, scale_down])
        all_scales = [scales] + [swap(scales, "fs", fs, mask) for mask in range(1, fs)]
        out_mine, out_other = gather_weight(weight_out.astype(jnp.bfloat16), 0, fs)
        up_mine, up_other = gather_weight(weight_up.astype(jnp.bfloat16), 1, fs, relay=True)
        down_mine, down_other = gather_weight(weight_down.astype(jnp.bfloat16), 0, fs, relay=True, whole_near=True)

        normed_in = normed_blocks(token_blocks, norm1_gain, fs, tp)
        full_u = jnp.concatenate(
            [jnp.concatenate([a[:, 0], b[:, 0]], axis=1) for a, b in zip(both_mine, both_other)]
        )
        full_v = jnp.concatenate(
            [jnp.concatenate([a[:, 1], b[:, 1]], axis=1) for a, b in zip(both_mine, both_other)]
        )
        pre_v = jnp.dot(normed_in, full_v, preferred_element_type=jnp.float32)
        pre_u = jnp.dot(normed_in, full_u, preferred_element_type=jnp.float32)
        act_v = jax.nn.gelu(pre_v * halves_swapped(scale_v, 0))
        gate_u = jax.nn.gelu(pre_u * halves_swapped(scale_u, 0))
        local_width = 2 * half
        row_sums, row_squares = lax.psum(
            (jnp.sum(act_v, axis=1), jnp.sum(act_v * act_v, axis=1)), "tp"
        )
        row_mean = (row_sums / GM_W)[:, None]
        square = (row_squares / GM_W)[:, None]
        v_norm = (
            (act_v - row_mean)
            * lax.rsqrt(square - row_mean * row_mean + 1e-06)
            * halves_swapped(mix_gain, 0)
        ).astype(jnp.bfloat16)
        group_index = lax.axis_index("tp") * local_width // (GM_W // GROUPS)
        lower_mask = jnp.tril(jnp.ones((BLOCK, BLOCK), jnp.float32))
        spatial_mask = (
            lax.dynamic_index_in_dim(spatial_weight, group_index, 0, keepdims=False) * lower_mask
        ).astype(jnp.bfloat16)
        block_bias = lax.dynamic_index_in_dim(spatial_bias, group_index, 0, keepdims=False)
        blocks = v_norm.reshape(-1, BLOCK, local_width)
        mixed = jnp.einsum("ts,nsc->ntc", spatial_mask, blocks, preferred_element_type=jnp.float32)
        mixed = mixed + block_bias[None, :, None]
        gated = (gate_u * mixed.reshape(-1, local_width)).astype(jnp.bfloat16)

        terms = []
        for a, b, scale in zip(out_mine, out_other, all_scales):
            product = jnp.dot(gated, jnp.concatenate([a, b]), preferred_element_type=jnp.float32)
            terms.append((product * scale[0]).astype(jnp.bfloat16))
        mixer_sum = scatter_sum(terms, fs, tp)
        residual = (tokens.astype(jnp.float32) + mixer_sum).astype(jnp.bfloat16)

        normed_mid = normed_blocks(gather_rows(residual, tp), norm2_gain, fs, tp)
        full_up = jnp.concatenate(
            [jnp.concatenate([a, b], axis=1) for a, b in zip(up_mine, up_other)]
        )
        pre_up = jnp.dot(normed_mid, full_up, preferred_element_type=jnp.float32)
        hidden = jnp.square(jax.nn.relu(pre_up * halves_swapped(scale_up, 0))).astype(jnp.bfloat16)
        terms = []
        for a, b, scale in zip(down_mine, down_other, all_scales):
            product = jnp.dot(hidden, jnp.concatenate([a, b]), preferred_element_type=jnp.float32)
            terms.append((product * scale[1]).astype(jnp.bfloat16))
        channel_sum = scatter_sum(terms, fs, tp)
        return (residual.astype(jnp.float32) + channel_sum).astype(jnp.bfloat16)

    return layer


MESH = pl.DeviceIdType.MESH
WAVES = 6
CHUNKS = 4
STEP = 64


def rows_of(first, size, unit):
    return pl.ds(pl.multiple_of(first, unit), size)


def row_loop(first, count, step, body):
    def at(i, carry):
        body(rows_of(first + i * step, step, step))
        return carry

    lax.fori_loop(0, count // step, at, 0)


def matmul(a, b):
    return jnp.dot(a, b, preferred_element_type=jnp.float32)


def fused_kernel(
    tokens, weight_u, weight_v, weight_out, weight_up, weight_down,
    gain1, scale_u, scale_v, mix_gain, spatial_weight, spatial_bias,
    scale_out, scale_down, gain2, scale_up,
    result_out,
    result, stage, g_both, g_out, g_up, g_down, tok, mid, mid_end, normed, hidden, hidden_end,
    act_v, gate_u, gated, stat, stat_rows, scales, terms, core_in, core_end, x_out, x_in, x_end,
    load_sem, zs, zr, ys, yr, zos, zor, gs, gr, cs, cr, xs, xr, cs2, cr2, xs2, xr2,
    cs3, cr3, xs3, xr3, es, er, ps, pr, sts, strv, scs, scr,
):
    y, z, t = lax.axis_index("grp"), lax.axis_index("fs"), lax.axis_index("tp")
    other_y = 1 - y
    upper = z // 2
    planes = (z, 1 - z + 4 * upper, 2 - upper, 3 - 3 * upper)
    is_mid = (z == 1) | (z == 2)
    is_end = jnp.logical_not(is_mid)
    terms_end = tok
    inner = (t == 1) | (t == 2)
    outer = jnp.logical_not(inner)
    t1 = t + 1 - 2 * (t % 2)
    t2 = (t + 2) % 4
    t3 = (t1 + 2) % 4
    rows, fine = tokens.shape
    chunk = rows // CHUNKS
    width = weight_u.shape[1]
    hid = weight_up.shape[1]
    hhalf = hid // 2
    feature_count = gain1.shape[1]
    sends = []

    def remote(source, target, send, recv, **where):
        return pltpu.make_async_remote_copy(
            src_ref=source, dst_ref=target, send_sem=send, recv_sem=recv,
            device_id=where, device_id_type=MESH,
        )

    barrier = pltpu.get_barrier_semaphore()
    for p in planes[1:]:
        pl.semaphore_signal(barrier, inc=1, device_id={"fs": p}, device_id_type=MESH)
    pl.semaphore_signal(barrier, inc=1, device_id={"grp": other_y}, device_id_type=MESH)
    for u in (t1, t2, t3):
        pl.semaphore_signal(barrier, inc=1, device_id={"tp": u}, device_id_type=MESH)

    def load(source, slot, part=None):
        target = stage.at[slot] if part is None else part
        return pltpu.make_async_copy(source, target, load_sem.at[slot])

    half_w = width
    load_u = load(weight_u, 0, stage.at[0, :, pl.ds(0, half_w)])
    load_v = pltpu.make_async_copy(weight_v, stage.at[0, :, pl.ds(half_w, half_w)], load_sem.at[4])
    load_out = load(weight_out, 1, stage.at[1, pl.ds(0, width), :])
    load_tok = pltpu.make_async_copy(tokens, tok.at[t], load_sem.at[5])

    def load_up(j, slot):
        return load(weight_up.at[:, pl.ds(j * fine, fine)], slot)

    def load_down(j, slot):
        return load(weight_down.at[pl.ds(j * fine, fine), :], slot)

    load_u.start()
    load_v.start()
    load_out.start()
    load_up(0, 2).start()
    load_up(1, 3).start()
    load_tok.start()
    scales[z] = jnp.concatenate([scale_out[...], scale_down[...]], axis=0)

    pl.semaphore_wait(barrier, 7)

    def gather_copies(which, buffer, own_source, r):
        part = pl.ds(r * chunk, chunk)
        to_x = remote(own_source.at[part], buffer.at[t, part], gs.at[which, 0, r], gr.at[which, t, r], tp=t2)
        to_core = remote(own_source.at[part], buffer.at[t, part], gs.at[which, 1, r], gr.at[which, t, r], tp=t1)
        return to_x, to_core

    def gather_start(which, buffer, own_source, r):
        for copy in gather_copies(which, buffer, own_source, r):
            copy.start()
            sends.append(copy)

    def gather_await(which, buffer, block, r):
        part = pl.ds(r * chunk, chunk)
        remote(buffer.at[block, part], buffer.at[block, part], gs.at[which, 2, r], gr.at[which, block, r], tp=t1).wait_recv()

    def relay_copy(which, buffer, r):
        part = pl.ds(r * chunk, chunk)
        return remote(buffer.at[t2, part], buffer.at[t2, part], gs.at[which, 2, r], gr.at[which, t2, r], tp=t1)

    def gather_relay(which, buffer, r, listed=True):
        gather_await(which, buffer, t2, r)
        copy = relay_copy(which, buffer, r)
        copy.start()
        if listed:
            sends.append(copy)

    def piece(w, p, h):
        if w == 0:
            size = fine // 2
            return g_both.at[rows_of(p * fine + h * size, size, size), :]
        if w == 1:
            size = width // 2
            return g_out.at[p, rows_of(h * size, size, size), :]
        if w < 4:
            size = fine // 2
            return g_up.at[h, rows_of(p * fine + (w - 2) * size, size, size), :]
        size = hhalf // 2
        return g_down.at[p, rows_of(h * hhalf + (w - 4) * size, size, size), :]

    def z_copy(w, p, to, slot):
        return remote(piece(w, p, y), piece(w, p, y), zs.at[w, slot], zr.at[w, p], fs=to)

    def y_copy(w, i, h):
        p = planes[i]
        return remote(piece(w, p, h), piece(w, p, h), ys.at[w, i - 1], yr.at[w, p], grp=other_y)

    def own(w):
        z_copy(w, z, planes[1], 0).start()

        @pl.when(is_mid)
        def _():
            z_copy(w, z, planes[2], 1).start()

    def arrive(w, i, cross=True):
        p = planes[i]
        z_copy(w, p, planes[1], 1 + i).wait_recv()

        @pl.when(is_mid)
        def _():
            z_copy(w, p, planes[2] if i == 1 else planes[1], 1 + i).start()

        if cross:
            y_copy(w, i, y).start()

    def arrive_y(w, i):
        y_copy(w, i, other_y).wait_recv()

    def arrive_all_y(w):
        for i in (1, 2, 3):
            arrive_y(w, i)

    def other_half(w, p):
        return remote(piece(w, p, other_y), piece(w, p, other_y), zos.at[w], zor.at[w], fs=planes[1])

    def own_end(w, first):
        @pl.when(is_end)
        def _():
            (z_copy(w, z, planes[1], 0) if first else other_half(w, z)).start()

    def own_mid(w):
        @pl.when(is_mid)
        def _():
            z_copy(w, z, planes[2], 1).start()

    def pass_on(w, i):
        @pl.when(is_mid)
        def _():
            p = planes[i]
            z_copy(w, p, planes[1], 1 + i).wait_recv()
            if i == 1:
                z_copy(w, p, planes[2], 2).start()
            else:
                y_copy(w, i, y).start()

    for r in range(CHUNKS):
        gather_start(0, tok, tokens, r)

    def cast_to(slot, count, store):
        row_loop(0, count, STEP, lambda part: store(part, stage[slot, part, :].astype(jnp.bfloat16)))

    def at_offset(part, base):
        return rows_of(part.start + base, part.size, part.size)

    load_u.wait()
    load_v.wait()

    def store_both(part, value):
        g_both[at_offset(part, z * fine), :] = value

    cast_to(0, fine, store_both)
    load_up(2, 0).start()
    load_out.wait()

    def store_out(part, value):
        g_out[z, part, :] = value

    own(0)
    cast_to(1, width, store_out)
    load_up(3, 1).start()
    for i in (1, 2, 3):
        copy = remote(scales.at[z], scales.at[z], scs.at[i - 1], scr.at[z], fs=planes[i])
        copy.start()
        sends.append(copy)

    def cast_up(j, slot):
        load_up(j, slot).wait()
        cols = pl.ds((j % 2) * fine, fine)

        def store(part, value):
            g_up[j // 2, at_offset(part, z * fine), cols] = value

        cast_to(slot, fine, store)

    def cast_down(j, slot):
        load_down(j, slot).wait()

        def store(part, value):
            g_down[z, at_offset(part, j * fine), :] = value

        cast_to(slot, fine, store)

    cast_up(0, 2)
    load_down(0, 2).start()
    cast_up(1, 3)
    load_down(1, 3).start()
    arrive(0, 1)
    own(1)
    cast_up(2, 0)
    load_down(2, 0).start()
    cast_up(3, 1)
    load_down(3, 1).start()
    own_end(2, True)
    own_end(3, True)
    own_mid(2)
    arrive(0, 2)
    gather_relay(0, tok, 0)
    arrive(0, 3)
    gather_relay(0, tok, 1)
    cast_down(0, 2)
    cast_down(1, 3)
    cast_down(2, 0)
    cast_down(3, 1)
    gather_relay(0, tok, 2)
    arrive(1, 1, False)
    arrive(1, 2, False)
    own_end(2, False)
    own_end(3, False)
    load_tok.wait()

    def norm_rows(buffer, gain, first, count):
        def body(part):
            total = jnp.zeros((part.size, 1), jnp.float32)
            for b in range(4):
                value = buffer[b, part, :].astype(jnp.float32)
                total = total + jnp.sum(value * value, axis=1, keepdims=True)
            inverse = lax.rsqrt(total / feature_count + 1e-06)
            for b in range(4):
                value = buffer[b, part, :].astype(jnp.float32)
                cols = pl.ds(b * fine, fine)
                normed[part, cols] = (value * inverse * gain[:, cols]).astype(jnp.bfloat16)

        row_loop(first, count, 32, body)

    def norm_chunk(which, buffer, gain, r):
        gather_await(which, buffer, t1, r)
        gather_await(which, buffer, t3, r)
        norm_rows(buffer, gain, r * chunk, chunk)

    for r in range(CHUNKS):
        if r == CHUNKS - 1:
            gather_relay(0, tok, r)
        norm_chunk(0, tok, gain1, r)

    own_mid(3)
    arrive_all_y(0)
    y_copy(1, 1, y).start()
    y_copy(1, 2, y).start()

    lane = lax.broadcasted_iota(jnp.int32, (chunk, 128), 1)

    def v_chunk(part):
        value = jax.nn.gelu(matmul(normed[part, :], g_both[:, width:]) * scale_v[...])
        act_v[part, :] = value
        total = jnp.sum(value, axis=1, keepdims=True)
        square = jnp.sum(value * value, axis=1, keepdims=True)
        stat[part, :] = jnp.where(lane == 0, total, jnp.where(lane == 1, square, 0.0))

    row_loop(0, rows, chunk, v_chunk)
    stat_rows[0] = stat[...].T[0:8]

    def stat_copy(k, u):
        return remote(stat_rows.at[0], stat_rows.at[k], sts.at[k - 1], strv.at[k], tp=u)

    def u_chunk(part):
        gate_u[part, :] = jax.nn.gelu(matmul(normed[part, :], g_both[:, :width]) * scale_u[...])

    for k, u in ((1, t1), (2, t2), (3, t3)):
        copy = stat_copy(k, u)
        copy.start()
        sends.append(copy)
    arrive(1, 3)
    row_loop(0, rows, chunk, u_chunk)
    for k, u in ((1, t1), (2, t2), (3, t3)):
        stat_copy(k, u).wait_recv()
    totals = stat_rows[0] + stat_rows[1] + stat_rows[2] + stat_rows[3]
    stat[...] = jnp.concatenate([totals, jnp.zeros((120, rows), jnp.float32)], axis=0).T

    down_at = lax.broadcasted_iota(jnp.int32, (BLOCK, BLOCK), 0)
    along = lax.broadcasted_iota(jnp.int32, (BLOCK, BLOCK), 1)
    mask = jnp.where(along <= down_at, spatial_weight[t], 0.0).astype(jnp.bfloat16)
    bias_row = spatial_bias[pl.ds(t, 1), :]
    bias = jnp.sum(jnp.where(along == down_at, bias_row, 0.0), axis=1, keepdims=True)

    def mix_block(part):
        mean = stat[part, 0:1] / GM_W
        square = stat[part, 1:2] / GM_W
        v_norm = (act_v[part, :] - mean) * lax.rsqrt(square - mean * mean + 1e-06) * mix_gain[...]
        mixed = matmul(mask, v_norm.astype(jnp.bfloat16)) + bias
        gated[part, :] = (gate_u[part, :] * mixed).astype(jnp.bfloat16)

    row_loop(0, rows, BLOCK, mix_block)
    pass_on(2, 1)
    own_end(4, True)
    arrive_all_y(1)
    for i in (1, 2, 3):
        remote(scales.at[planes[i]], scales.at[planes[i]], scs.at[i - 1], scr.at[planes[i]], fs=planes[i]).wait_recv()

    def core_copy(k, block, r):
        part = pl.ds(r * chunk, chunk)
        return remote(terms.at[block, part], core_in.at[k, part], cs.at[k, r], cr.at[k, r], tp=t1)

    def x_copy(send, recv, r):
        part = pl.ds(r * chunk, chunk)
        return remote(x_out.at[part], x_in.at[part], send.at[r], recv.at[r], tp=t2)

    def end_copy(r):
        part = pl.ds(r * chunk, chunk)
        return remote(mid.at[t, part], mid_end.at[t, part], gs.at[1, 0, r], gr.at[2, t, r], fs=planes[1])

    pass_on(2, 2)
    mix_sends = []
    for r in range(CHUNKS):
        part = pl.ds(r * chunk, chunk)
        for j in range(4):
            product = matmul(gated[part, :], g_out[j])
            terms[j, part, :] = (product * scales[j, 0:1, :]).astype(jnp.bfloat16)
        for k, block in ((0, t1), (1, t3)):
            copy = core_copy(k, block, r)
            copy.start()
            mix_sends.append(copy)

    def pair_out(block, slot, r):
        def body(part):
            both = terms[block, part, :].astype(jnp.float32) + core_in[slot, part, :].astype(jnp.float32)
            x_out[part, :] = both.astype(jnp.bfloat16)

        row_loop(r * chunk, chunk, STEP, body)

    for r in range(CHUNKS):
        core_copy(0, t1, r).wait_recv()
        core_copy(1, t3, r).wait_recv()
        pair_out(t2, 1, r)
        copy = x_copy(xs, xr, r)
        copy.start()
        mix_sends.append(copy)
    pass_on(3, 1)
    own_mid(4)

    for r in range(CHUNKS):
        x_copy(xs, xr, r).wait_recv()

        def residual_rows(part):
            total = terms[t, part, :].astype(jnp.float32) + core_in[0, part, :].astype(jnp.float32)
            total = total + x_in[part, :].astype(jnp.float32)
            mid[t, part, :] = (tok[t, part, :].astype(jnp.float32) + total).astype(jnp.bfloat16)

        row_loop(r * chunk, chunk, STEP, residual_rows)

        @pl.when(is_mid)
        def _():
            for copy in gather_copies(1, mid, mid.at[t], r):
                copy.start()

        @pl.when(is_end)
        def _():
            end_copy(r).start()

        if r == 0:
            pass_on(3, 2)
        if r == 2:
            pass_on(2, 3)

    for copy in sends + mix_sends:
        copy.wait_send()

    tile = min(hhalf, fine)

    def up_half(target, h, first=0, count=rows):
        def body(part):
            for n in range(hhalf // tile):
                cols = pl.ds(n * tile, tile)
                place = rows_of(h * hhalf + n * tile, tile, 128)
                value = matmul(normed[part, :], g_up[h, :, cols]) * scale_up[:, place]
                value = jnp.maximum(value, 0.0)
                target[part, place] = (value * value).astype(jnp.bfloat16)

        row_loop(first, count, chunk, body)

    sets = {
        True: (hidden, terms, core_in, cs2, cr2),
        False: (hidden_end, terms_end, core_end, cs3, cr3),
    }

    def chan_core(near, i, r):
        _, out, into, send, recv = sets[near]
        j = planes[i]
        part = rows_of(r * chunk, chunk, chunk)
        return remote(out.at[j, part], into.at[j // 2, part], send.at[i, r], recv.at[j // 2, r], tp=t1)

    def end_x_copy(slot, r):
        part = pl.ds(r * chunk, chunk)
        return remote(core_end.at[slot, part], x_end.at[part], xs3.at[r], xr3.at[r], tp=t2)

    def pair_copy(slot, r):
        part = pl.ds(r * chunk, chunk)
        return remote(core_end.at[slot, part], core_in.at[slot, part], ps.at[r], pr.at[r], fs=planes[1])

    def end_swap(slot, r):
        part = pl.ds(r * chunk, chunk)
        return remote(core_in.at[slot, part], x_in.at[part], xs2.at[r], xr2.at[r], tp=t2)

    def back_copy(r):
        part = pl.ds(r * chunk, chunk)
        return remote(x_end.at[part], x_in.at[part], es.at[r], er.at[r], fs=planes[1])

    def down_dots(near, i):
        source, out = sets[near][:2]
        j = planes[i]
        mine = (j % 2) == (t % 2)

        def one(r, carry):
            part = rows_of(r * chunk, chunk, chunk)
            product = matmul(source[part, :], g_down[j])
            out[j, part, :] = (product * scales[j, 1:2, :]).astype(jnp.bfloat16)

            @pl.when(jnp.logical_not(mine))
            def _():
                chan_core(near, i, r).start()

            return carry

        lax.fori_loop(0, CHUNKS, one, 0)

    def pair_up(near, i):
        j = planes[i]
        slot = j // 2

        @pl.when((j % 2) == (t % 2))
        def _():
            for r in range(CHUNKS):
                chan_core(near, i, r).wait_recv()
                if near:
                    @pl.when(j != t)
                    def _():
                        pair_out(j, slot, r)
                        x_copy(xs2, xr2, r).start()
                else:
                    def body(part):
                        both = tok[j, part, :].astype(jnp.float32) + core_end[slot, part, :].astype(jnp.float32)
                        core_end[slot, part, :] = both.astype(jnp.bfloat16)

                    if i in (0, 2):
                        row_loop(r * chunk, chunk, STEP, body)
                        pair_copy(slot, r).start()
                    else:
                        @pl.when(j != t)
                        def _():
                            row_loop(r * chunk, chunk, STEP, body)
                            end_x_copy(slot, r).start()

    def store_copy(r):
        part = pl.ds(r * chunk, chunk)
        return pltpu.make_async_copy(result.at[part], result_out.at[part], load_sem.at[r])

    def finish_end(i):
        @pl.when(planes[i] == t)
        def _():
            for r in range(CHUNKS):
                end_x_copy(t2 // 2, r).wait_recv()

                def end_rows(part):
                    total = tok[t, part, :].astype(jnp.float32) + core_end[t // 2, part, :].astype(jnp.float32)
                    total = total + x_end[part, :].astype(jnp.float32)
                    x_end[part, :] = (mid_end[t, part, :].astype(jnp.float32) + total).astype(jnp.bfloat16)

                row_loop(r * chunk, chunk, STEP, end_rows)
                back_copy(r).start()

    @pl.when(is_mid)
    def _():
        own_mid(5)

        def up_chunks(target, first, count):
            for h in (0, 1):
                up_half(target, h, first * chunk, count * chunk)

        def near_chunk(r):
            gather_relay(1, mid, r, False)
            norm_chunk(1, mid, gain2, r)

        def end_send(r):
            gather_await(2, mid_end, t, r)
            for copy in gather_copies(2, mid_end, mid_end.at[t], r):
                copy.start()

        def end_chunk(r):
            norm_chunk(2, mid_end, gain2, r)
            up_chunks(hidden_end, r, 1)

        pass_on(3, 3)
        near_chunk(0)
        near_chunk(1)
        up_half(hidden, y, 0, 2 * chunk)
        pass_on(4, 2)
        near_chunk(2)
        end_send(0)
        end_send(1)
        for w in (2, 3):
            other_half(w, planes[1]).wait_recv()
            arrive_y(w, 2)
            arrive_y(w, 3)
        up_half(hidden, other_y, 0, 2 * chunk)
        pass_on(4, 1)
        end_send(2)
        up_chunks(hidden, 2, 1)
        near_chunk(3)
        pass_on(5, 2)
        up_chunks(hidden, 3, 1)
        end_send(3)
        gather_relay(2, mid_end, 0, False)
        down_dots(True, 0)
        end_chunk(0)
        gather_relay(2, mid_end, 1, False)
        pass_on(5, 1)
        end_chunk(1)
        gather_relay(2, mid_end, 2, False)
        pair_up(True, 0)
        pass_on(4, 3)
        for w in (4, 5):
            arrive_y(w, 2)
        down_dots(True, 2)
        gather_relay(2, mid_end, 3, False)
        end_chunk(2)
        pair_up(True, 2)
        pass_on(5, 3)
        end_chunk(3)
        down_dots(False, 0)
        down_dots(False, 2)
        pair_up(False, 0)
        for w in (4, 5):
            other_half(w, planes[1]).wait_recv()
        down_dots(False, 1)
        pair_up(False, 2)
        down_dots(True, 1)
        pair_up(False, 1)
        for w in (4, 5):
            arrive_y(w, 3)
        down_dots(False, 3)
        pair_up(True, 1)
        pair_up(False, 3)
        down_dots(True, 3)
        pair_up(True, 3)
        for i in (1, 3):
            finish_end(i)
        for r in range(CHUNKS):
            x_copy(xs2, xr2, r).wait_recv()

            def result_rows(part):
                total = terms[t, part, :].astype(jnp.float32) + core_in[t // 2, part, :].astype(jnp.float32)
                total = total + x_in[part, :].astype(jnp.float32)
                result[part, :] = (mid[t, part, :].astype(jnp.float32) + total).astype(jnp.bfloat16)

            row_loop(r * chunk, chunk, STEP, result_rows)
            store_copy(r).start()

    @pl.when(is_end)
    def _():
        z_copy(5, z, planes[1], 0).start()
        z_copy(5, z, planes[1], 0).wait_send()
        for w in (4, 5):
            other_half(w, z).start()
        near_slot = 1 - t % 2
        for r in range(CHUNKS):
            pair_copy(near_slot, r).wait_recv()

            @pl.when(outer)
            def _():
                end_swap(near_slot, r).start()

        @pl.when(inner)
        def _():
            for r in range(CHUNKS):
                end_swap(near_slot, r).wait_recv()

                def sum_rows(part):
                    total = core_in[near_slot, part, :].astype(jnp.float32) + x_in[part, :].astype(jnp.float32)
                    result[part, :] = (mid[t, part, :].astype(jnp.float32) + total).astype(jnp.bfloat16)

                row_loop(r * chunk, chunk, STEP, sum_rows)
                store_copy(r).start()

        @pl.when(outer)
        def _():
            for r in range(CHUNKS):
                back_copy(r).wait_recv()

                def take_rows(part):
                    result[part, :] = x_in[part, :]

                row_loop(r * chunk, chunk, STEP, take_rows)
                store_copy(r).start()
                end_swap(near_slot, r).wait_send()

    for r in range(CHUNKS):
        store_copy(r).wait()
    for w in (0, 1):
        z_copy(w, z, planes[1], 0).wait_send()
        for i in (1, 2, 3):
            y_copy(w, i, y).wait_send()

    @pl.when(is_end)
    def _():
        for w in range(2, WAVES):
            if w < 5:
                z_copy(w, z, planes[1], 0).wait_send()
            other_half(w, z).wait_send()
        for r in range(CHUNKS):
            end_copy(r).wait_send()

    @pl.when(is_mid)
    def _():
        for w in (0, 1):
            z_copy(w, z, planes[2], 1).wait_send()
            for i in (1, 2, 3):
                z_copy(w, planes[i], planes[1], 1 + i).wait_send()
        for w in range(2, WAVES):
            z_copy(w, z, planes[2], 1).wait_send()
            z_copy(w, planes[1], planes[2], 2).wait_send()
            for i in (2, 3):
                y_copy(w, i, y).wait_send()
        for r in range(CHUNKS):
            x_copy(xs2, xr2, r).wait_send()
            for which, buffer in ((1, mid), (2, mid_end)):
                for copy in gather_copies(which, buffer, buffer.at[t], r):
                    copy.wait_send()
                relay_copy(which, buffer, r).wait_send()
            pair_copy(1 - t % 2, r).wait_send()

            @pl.when(inner)
            def _():
                end_x_copy(t2 // 2, r).wait_send()

            @pl.when(outer)
            def _():
                back_copy(r).wait_send()
        for i in range(4):
            @pl.when((planes[i] % 2) != (t % 2))
            def _():
                for r in range(CHUNKS):
                    chan_core(True, i, r).wait_send()
                    chan_core(False, i, r).wait_send()


def fused_layer(
    tokens, norm1_gain, weight_u, weight_v, scale_u, scale_v, mix_gain, spatial_weight,
    spatial_bias, weight_out, scale_out, norm2_gain, weight_up, scale_up, weight_down, scale_down,
):
    rows, fine = tokens.shape
    depth, width, hid = norm1_gain.shape[0], weight_u.shape[1], weight_up.shape[1]
    bf16, f32 = jnp.bfloat16, jnp.float32
    vmem = lambda shape, kind: pltpu.VMEM(shape, kind)
    dma = lambda *shape: pltpu.SemaphoreType.DMA(shape)
    row = lambda value: value[None, :]
    hbm = pl.BlockSpec(memory_space=pl.ANY)
    local = pl.BlockSpec(memory_space=pltpu.VMEM)
    return pl.pallas_call(
        fused_kernel,
        name="fused_layer",
        out_shape=jax.ShapeDtypeStruct((rows, fine), bf16),
        in_specs=[hbm] * 6 + [local] * 10,
        out_specs=hbm,
        scratch_shapes=[
            vmem((rows, fine), bf16),
            vmem((4, fine, fine), f32),
            vmem((depth, 2 * width), bf16),
            vmem((4, width, fine), bf16),
            vmem((2, depth, hid // 2), bf16),
            vmem((4, hid, fine), bf16),
            vmem((4, rows, fine), bf16),
            vmem((4, rows, fine), bf16),
            vmem((4, rows, fine), bf16),
            vmem((rows, depth), bf16),
            vmem((rows, hid), bf16),
            vmem((rows, hid), bf16),
            vmem((rows, width), f32),
            vmem((rows, width), f32),
            vmem((rows, width), bf16),
            vmem((rows, 128), f32),
            vmem((4, 8, rows), f32),
            vmem((4, 2, fine), f32),
            vmem((4, rows, fine), bf16),
            vmem((2, rows, fine), bf16),
            vmem((2, rows, fine), bf16),
            vmem((rows, fine), bf16),
            vmem((rows, fine), bf16),
            vmem((rows, fine), bf16),
            dma(6),
            dma(WAVES, 5), dma(WAVES, 4), dma(WAVES, 3), dma(WAVES, 4), dma(WAVES), dma(WAVES),
            dma(3, 3, CHUNKS), dma(3, 4, CHUNKS),
            dma(2, CHUNKS), dma(2, CHUNKS), dma(CHUNKS), dma(CHUNKS),
            dma(4, CHUNKS), dma(2, CHUNKS), dma(CHUNKS), dma(CHUNKS),
            dma(4, CHUNKS), dma(2, CHUNKS), dma(CHUNKS), dma(CHUNKS), dma(CHUNKS), dma(CHUNKS), dma(CHUNKS), dma(CHUNKS),
            dma(3), dma(4), dma(3), dma(4),
        ],
        compiler_params=pltpu.CompilerParams(
            collective_id=0, has_side_effects=True, vmem_limit_bytes=67043328
        ),
    )(
        tokens, weight_u, weight_v, weight_out, weight_up, weight_down,
        row(norm1_gain), row(scale_u), row(scale_v), row(mix_gain), spatial_weight, spatial_bias,
        row(scale_out), row(scale_down), row(norm2_gain), row(scale_up),
    )


def solution(mesh):
    placed = (
        P(("grp", "fs"), "tp"),
        P(),
        P("fs", "tp"),
        P("fs", "tp"),
        P("tp"),
        P("tp"),
        P("tp"),
        P(),
        P(),
        P("tp", "fs"),
        P("fs"),
        P(),
        P("fs", "tp"),
        P("tp"),
        P("tp", "fs"),
        P("fs"),
    )
    grp, fs, tp = mesh.shape["grp"], mesh.shape["fs"], mesh.shape["tp"]
    fused = grp == 2 and fs == 4 and tp == 4
    return jax.shard_map(
        fused_layer if fused else make(fs, tp),
        mesh=mesh,
        in_specs=placed,
        out_specs=P(("grp", "fs"), "tp"),
        check_vma=False,
    )
```
